32 devices in a mesh: ep: 8 (over z, y), tp: 4 (over x, core).
Axes of the slice: x: 2, y: 2, z: 4, core: 2. Of those that a mesh axis runs over, the one named last changes fastest.
Arguments:
- value_in: bfloat16 [4096, 2048], P('ep', 'tp'), may hold values from -400 to 400
- gate_in: bfloat16 [4096, 2048], P('ep', 'tp'), may hold values from -8 to 8
- conv_taps: float32 [31, 2048], P(None, 'tp'), may hold values from -1 to 1
- conv_bias: float32 [2048], P('tp'), may hold values from -3 to 3
- ln_gain: float32 [2048], P('tp'), may hold values from 0.1 to 1.9
- ln_bias: float32 [2048], P('tp'), may hold values from -3 to 3
- out_proj: bfloat16 [2048, 4096], P('tp'), may hold values from -0.125 to 0.125
- tokens_b: bfloat16 [4096, 4096], P('ep'), may hold values from -6 to 6
- norm_gain: float32 [4096], replicated, may hold values from 0.1 to 1.9
- routes: int32 [4096, 2], P(('ep', 'tp')), may hold values from 0 to 7, all different within a row; in each aligned block of 128 rows (0 to 127, 128 to 255, ...) at most 48 rows name the same one
- route_weights: float32 [4096, 2], P(('ep', 'tp')), may hold values from 0.2 to 1.5
- expert_gate: bfloat16 [8, 4096, 1024], P('ep', None, 'tp'), may hold values from -0.09375 to 0.09375
- expert_up: bfloat16 [8, 4096, 1024], P('ep', None, 'tp'), may hold values from -0.09375 to 0.09375
- expert_down: bfloat16 [8, 1024, 4096], P('ep', 'tp'), may hold values from -0.1875 to 0.1875
- shared_gate: bfloat16 [4096, 1024], P(None, 'tp'), may hold values from -0.09375 to 0.09375
- shared_up: bfloat16 [4096, 1024], P(None, 'tp'), may hold values from -0.09375 to 0.09375
- shared_down: bfloat16 [1024, 4096], P('tp'), may hold values from -0.1875 to 0.1875
Outputs:
- mixer_out: bfloat16 [4096, 4096], P(('ep', 'tp'))
- experts_out: bfloat16 [4096, 4096], P(('ep', 'tp'))
The draws below stay inside these ranges and needn't reach their ends.
Inputs may be any that keep to these rules, and one draw needn't show every extreme that they name: `routes`: each row names 2 different experts. In each aligned block of 128 rows (the rows of one device) no expert is named by more than 48 rows, and in some blocks an expert is named by exactly 48 rows.
All inputs are finite; a program needn't handle non-finite values.
Results may differ from the reference program's by a relative error of at most 0.012.
Values may be sent and summed in bfloat16 or wider, within the bound.
A program may use at most 128 MiB of HBM per device.

```python
import math
from functools import partial
import jax
import jax.numpy as jnp
import numpy as np
from jax import lax

D = 4096
CHANNELS = 2048
EXPERT_WIDTH = 1024
TAPS = 31
TOP_K = 2
ROWS_DEV = 128
EXPERTS = 8
CAP = 48
SEQ_LEN = 4096
TOKENS_B = 4096
N_TP = 4


def draw_value_in(key, part):
    keys = jax.random.split(jax.random.fold_in(key, 11), 2)
    base = jnp.clip(jax.random.normal(keys[0], (SEQ_LEN, CHANNELS), jnp.float32), -5.0, 5.0)
    column = jnp.arange(CHANNELS, dtype=jnp.float32) / CHANNELS
    rough = jax.random.uniform(keys[1], (CHANNELS,), jnp.float32, 0.5, 1.5)
    scales = 0.3 * 10.0 ** column * rough
    values = base * scales[None, :]
    return values.astype(jnp.bfloat16)


def levels(key, dims, shards, least, largest):
    gain, own = 1.0, jax.random.fold_in(key, 6)
    for position, shards_of in shards:
        draws = jnp.exp(jax.random.uniform(jax.random.fold_in(own, position), (shards_of,), jnp.float32, least / len(shards), largest / len(shards)))
        gain = gain * jnp.repeat(draws, dims[position] // shards_of).reshape([-1 if axis == position else 1 for axis in range(len(dims))])
    return gain


def deal_out(rng, own, number, rows, amount, top, limit, lean):
    order = jax.random.permutation(rng, amount)
    heavy_load, ordinary = load_shares(amount, rows * top, limit, lean, True), load_shares(amount, rows * top, limit, lean, False)
    places = jnp.arange(amount)

    def named(sizes, offset_by):
        used = int((sizes > 0).sum())
        fixed = max(1, used // 4)
        shifted = fixed + (places - fixed + offset_by * (used - fixed)) % max(1, amount - fixed)
        return jnp.zeros((amount,), jnp.int32).at[order[jnp.where(places < fixed, places, shifted)]].set(jnp.asarray(sizes, jnp.int32))

    sizes = jnp.where(number % 4 == 0, named(heavy_load, number // 4), named(ordinary, number - number // 4 - 1))
    mixed = jax.random.permutation(jax.random.fold_in(own, 3), amount)
    giver, sink = mixed[0:amount // 2 * 2:2], mixed[1:amount // 2 * 2:2]
    slack = jnp.minimum(sizes[giver] - 1, limit - sizes[sink]) // 2
    slack = jnp.where((giver == order[0]) | (sink == order[0]) | (sizes[sink] == 0), 0, jnp.maximum(slack, 0))
    shifted = jax.random.randint(jax.random.fold_in(own, 4), (amount // 2,), 0, 1 << 20) % (slack + 1)
    sizes = sizes.at[giver].add(-shifted).at[sink].add(shifted)
    labels = jnp.searchsorted(jnp.cumsum(sizes), jnp.arange(rows * top), side="right").astype(jnp.int32)
    table = labels.reshape(top, rows).T
    table = table[jax.random.permutation(jax.random.fold_in(own, 1), rows)]
    offset_by = jax.random.randint(jax.random.fold_in(own, 2), (rows, 1), 0, top)
    return jnp.take_along_axis(table, (jnp.arange(top)[None, :] + offset_by) % top, axis=1)


def load_shares(number_of, total, most, lean, full):
    portions = [(1 << 20) // math.isqrt(rank ** lean) + 1 for rank in range(1, number_of + 1)]
    largest = most if full else min(most, max(-(-total // number_of), total * portions[0] // sum(portions)))
    least = 1 if total - largest >= number_of - 1 else 0
    holding, rest = [largest] + [least] * (number_of - 1), total - largest - least * (number_of - 1)
    while rest > 0:
        free = [i for i in range(1, number_of) if holding[i] < largest] or [i for i in range(1, number_of) if holding[i] < most]
        whole, left = sum([portions[i] for i in free]), rest
        for i in free:
            addition = min(most - holding[i], max(1, left * portions[i] // whole), rest)
            holding[i] = holding[i] + addition
            rest = rest - addition
    return np.array(holding)


def normal_values(key, dims, deviation, bound, pieces=(), kind=jnp.bfloat16):
    values = jax.random.normal(key, dims, jnp.float32) * deviation
    if len(pieces) > 0:
        values = levels(key, dims, pieces, -0.22, 0.18) * values
    return jnp.clip(values, min=-bound, max=bound).astype(kind)


def setup_inputs(seed: int = 0) -> dict:
    key_of = jax.random.split(jax.random.key(seed), 18)
    value_in = draw_value_in(jax.random.fold_in(key_of[17], 71), 0)
    gate_in = normal_values(key_of[1], (SEQ_LEN, CHANNELS), 1.5, 8.0, ((0, 8), (1, 4)))
    conv_taps = normal_values(key_of[2], (TAPS, CHANNELS), TAPS ** -0.5, 1.0, ((1, 4),), jnp.float32)
    conv_bias = normal_values(key_of[3], (CHANNELS,), 0.5, 3.0, ((0, 4),), jnp.float32)
    ln_gain = jnp.clip(1.0 + 0.18 * jax.random.normal(key_of[4], (CHANNELS,), jnp.float32), 0.1, 1.9)
    ln_bias = normal_values(key_of[5], (CHANNELS,), 0.5, 3.0, ((0, 4),), jnp.float32)
    out_proj = normal_values(key_of[6], (CHANNELS, D), CHANNELS ** -0.5, 0.125, ((0, 4),))
    tokens_b = normal_values(key_of[7], (TOKENS_B, D), 1.0, 6.0, ((0, 8),))
    norm_gain = jnp.clip(1.0 + 0.18 * jax.random.normal(key_of[8], (D,), jnp.float32), 0.1, 1.9)
    routes_keys = jax.random.split(jax.random.fold_in(key_of[9], 1), TOKENS_B // ROWS_DEV)
    routes_turns = jax.random.permutation(jax.random.fold_in(key_of[9], 3), TOKENS_B // ROWS_DEV)
    routes = jax.vmap(lambda own, number: deal_out(jax.random.fold_in(key_of[9], 2), own, number, ROWS_DEV, EXPERTS, TOP_K, CAP, 1))(routes_keys, routes_turns).reshape((TOKENS_B, TOP_K))
    route_weights = jnp.clip(0.2 + 1.3 * jax.random.uniform(key_of[10], (TOKENS_B, TOP_K), jnp.float32) ** levels(key_of[10], (TOKENS_B, TOP_K), ((0, 32),), -0.2, 0.2), 0.2, 1.5)
    expert_gate = normal_values(key_of[11], (EXPERTS, D, EXPERT_WIDTH), D ** -0.5, 0.09375, ((0, 8), (2, 4)))
    expert_up = normal_values(key_of[12], (EXPERTS, D, EXPERT_WIDTH), D ** -0.5, 0.09375, ((0, 8), (2, 4)))
    expert_down = normal_values(key_of[13], (EXPERTS, EXPERT_WIDTH, D), EXPERT_WIDTH ** -0.5, 0.1875, ((0, 8), (1, 4)))
    shared_gate = normal_values(key_of[14], (D, EXPERT_WIDTH), D ** -0.5, 0.09375, ((1, 4),))
    shared_up = normal_values(key_of[15], (D, EXPERT_WIDTH), D ** -0.5, 0.09375, ((1, 4),))
    shared_down = normal_values(key_of[16], (EXPERT_WIDTH, D), EXPERT_WIDTH ** -0.5, 0.1875, ((0, 4),))
    return dict(value_in=value_in, gate_in=gate_in, conv_taps=conv_taps, conv_bias=conv_bias, ln_gain=ln_gain, ln_bias=ln_bias, out_proj=out_proj, tokens_b=tokens_b, norm_gain=norm_gain, routes=routes, route_weights=route_weights, expert_gate=expert_gate, expert_up=expert_up, expert_down=expert_down, shared_gate=shared_gate, shared_up=shared_up, shared_down=shared_down)


EPSILON = 1e-06

def round_trip(values):
    return lax.optimization_barrier(values.astype(jnp.bfloat16)).astype(jnp.float32)

def blocked_product(hidden, weight):
    block_rows = hidden.shape[1] // N_TP
    summed = jnp.zeros((hidden.shape[0], weight.shape[1]), jnp.float32)
    for block in range(N_TP):
        partial_sum = jnp.dot(hidden[:, block * block_rows:(block + 1) * block_rows], weight[block * block_rows:(block + 1) * block_rows], preferred_element_type=jnp.float32)
        summed = summed + round_trip(partial_sum)
    return summed.astype(jnp.bfloat16)

def gated_ffn(rows_in, weight_gate, weight_up, weight_down):
    hidden = (jax.nn.silu(jnp.dot(rows_in, weight_gate, preferred_element_type=jnp.float32)) * jnp.dot(rows_in, weight_up, preferred_element_type=jnp.float32)).astype(jnp.bfloat16)
    return blocked_product(hidden, weight_down)

def slot_table(route_ids, expert_count):
    chosen = route_ids.reshape(-1)
    onehot = (chosen[:, None] == jnp.arange(expert_count, dtype=jnp.int32)[None, :]).astype(jnp.int32)
    earlier = jnp.cumsum(onehot, axis=0) - onehot
    return (chosen, lax.optimization_barrier(jnp.sum(earlier * onehot, axis=1)).astype(jnp.int32))

def reference(value_in, gate_in, conv_taps, conv_bias, ln_gain, ln_bias, out_proj, tokens_b, norm_gain, routes, route_weights, expert_gate, expert_up, expert_down, shared_gate, shared_up, shared_down):
    gated = round_trip(value_in.astype(jnp.float32) * jax.nn.sigmoid(gate_in.astype(jnp.float32)))
    padded = jnp.concatenate([jnp.zeros((TAPS - 1, CHANNELS), jnp.float32), gated], axis=0)
    filtered = jnp.zeros((SEQ_LEN, CHANNELS), jnp.float32) + conv_bias[None, :]
    for tap_index in range(TAPS):
        filtered = filtered + conv_taps[tap_index][None, :] * padded[tap_index:tap_index + SEQ_LEN]
    average = lax.optimization_barrier(jnp.sum(filtered, axis=1)) / CHANNELS
    variance = lax.optimization_barrier(jnp.sum(filtered * filtered, axis=1)) / CHANNELS - average * average
    normed_a = (filtered - average[:, None]) * lax.rsqrt(variance[:, None] + EPSILON) * ln_gain + ln_bias
    activated = jax.nn.silu(normed_a).astype(jnp.bfloat16)
    mixer_out = blocked_product(activated, out_proj)
    features = tokens_b.astype(jnp.float32)
    normed_b = (features * lax.rsqrt(lax.optimization_barrier(jnp.mean(features * features, axis=1, keepdims=True)) + EPSILON) * norm_gain).astype(jnp.bfloat16)
    block_count = TOKENS_B // ROWS_DEV
    chosen, places = jax.vmap(partial(slot_table, expert_count=EXPERTS))(routes.reshape(block_count, ROWS_DEV * TOP_K))
    row_ids = jnp.arange(block_count, dtype=jnp.int32)[:, None] * ROWS_DEV + jnp.arange(ROWS_DEV * TOP_K, dtype=jnp.int32)[None, :] // TOP_K
    block_grid = jnp.broadcast_to(jnp.arange(block_count, dtype=jnp.int32)[:, None], row_ids.shape)
    slot_rows = jnp.zeros((EXPERTS, block_count, CAP), jnp.int32).at[chosen, block_grid, places].set(row_ids)
    slot_weights = jnp.zeros((EXPERTS, block_count, CAP), jnp.float32).at[chosen, block_grid, places].set(route_weights.reshape(block_count, ROWS_DEV * TOP_K))

    def per_expert(accumulated, inputs):
        weight_gate, weight_up, weight_down, rows_expert, weights_expert = inputs
        picked_ids = rows_expert.reshape(-1)
        outputs = gated_ffn(normed_b[picked_ids], weight_gate, weight_up, weight_down)
        accumulated = accumulated.at[picked_ids].add(outputs.astype(jnp.float32) * weights_expert.reshape(-1)[:, None])
        return (accumulated, None)
    routed, _ = lax.scan(per_expert, jnp.zeros((TOKENS_B, D), jnp.float32), (expert_gate, expert_up, expert_down, slot_rows, slot_weights))
    shared_rows = gated_ffn(normed_b, shared_gate, shared_up, shared_down)
    experts_out = (shared_rows.astype(jnp.float32) + routed).astype(jnp.bfloat16)
    return (mixer_out, experts_out)
```

```python
import jax
import jax.numpy as jnp
from jax import lax
from jax.experimental import pallas as pl
from jax.experimental.pallas import tpu as pltpu
from jax.sharding import PartitionSpec as P


MESH = pl.DeviceIdType.MESH

EPSILON = 1e-06
COLUMN_CHUNKS = 4
TILE = 256
DEPTH = 1024
NEAR, FAR = 1, 2


def shifted(x, axis, by):
    devices = lax.axis_size(axis)
    pairs = [(i, i + by) for i in range(devices) if 0 <= i + by < devices]
    return lax.ppermute(x, axis, pairs)


def swapped(x, axis, bit):
    devices = lax.axis_size(axis)
    return lax.ppermute(x, axis, [(i, i ^ bit) for i in range(devices)])


def half_scattered(lhs, weight):
    count = lax.axis_size("tp")
    me = lax.axis_index("tp")
    rows, width = lhs.shape[0] // count, weight.shape[1]
    core, low = me % 2, me // 2
    blocks = lhs.reshape(count // 2, 2, rows, lhs.shape[1])
    sent = lax.dynamic_index_in_dim(blocks, 1 - core, 1, keepdims=False).reshape(-1, lhs.shape[1])
    kept = lax.dynamic_index_in_dim(blocks, core, 1, keepdims=False).reshape(-1, lhs.shape[1])
    sent = jnp.dot(sent, weight, preferred_element_type=jnp.float32).astype(jnp.bfloat16)
    arrived = swapped(sent, "tp", NEAR)
    kept = jnp.dot(kept, weight, preferred_element_type=jnp.float32).astype(jnp.bfloat16)
    halves = [part.reshape(count // 2, rows, width) for part in (kept, arrived)]
    give = sum(
        lax.dynamic_index_in_dim(h, 1 - low, 0, keepdims=False).astype(jnp.float32) for h in halves
    ).astype(jnp.bfloat16)
    keep = sum(
        lax.dynamic_index_in_dim(h, low, 0, keepdims=False).astype(jnp.float32) for h in halves
    )
    return give, keep


def expert_kernel(
    rows_ref,
    g0,
    g1,
    g2,
    g3,
    u0,
    u1,
    u2,
    down_ref,
    choice_ref,
    share_ref,
    give_s,
    give_m,
    keep_s,
    keep_m,
    mixer_ref,
    out_ref,
    wbuf,
    acc,
    hid,
    downs,
    prod,
    ret,
    arr,
    load_sem,
    relay_sem,
    down_send,
    down_recv,
    near_send,
    near_recv,
    rs_send,
    rs_recv,
    ret_send,
    ret_recv,
):
    me, t = lax.axis_index("ep"), lax.axis_index("tp")
    count = lax.axis_size("ep")
    chunks, _, cap, chunk = prod.shape
    near = {"tp": t + 1 - 2 * lax.rem(t, 2)}
    far = {"tp": lax.rem(t + 2, 4)}

    def remote(src, dst, send, recv, to):
        return pltpu.make_async_remote_copy(
            src_ref=src, dst_ref=dst, send_sem=send, recv_sem=recv, device_id=to, device_id_type=MESH
        )

    def cols(c):
        return pl.ds(c * chunk, chunk)

    barrier = pltpu.get_barrier_semaphore()
    pl.semaphore_signal(barrier, inc=1, device_id=near, device_id_type=MESH)
    pl.semaphore_signal(barrier, inc=1, device_id=far, device_id_type=MESH)

    @pl.loop(1, count)
    def _(j):
        pl.semaphore_signal(
            barrier, inc=1, device_id={"ep": lax.rem(me + j, count)}, device_id_type=MESH
        )

    loads = [
        pltpu.make_async_copy(src, wbuf.at[slot], load_sem.at[slot])
        for src, slot in ((g0, 0), (u0, 4), (g2, 2), (u2, 6), (g1, 1), (u1, 5), (g3, 3))
    ]
    for load in loads:
        load.start()
    pl.semaphore_wait(barrier, count + 1)

    to_far = [
        remote(
            down_ref.at[:, cols(c)], downs.at[0, :, cols(c)], down_send.at[c], down_recv.at[c], far
        )
        for c in range(chunks)
    ]
    relay = remote(u1, wbuf.at[7], relay_sem.at[0], relay_sem.at[1], near)
    to_near = [
        remote(
            down_ref.at[:, cols(c)],
            downs.at[1, :, cols(c)],
            near_send.at[0, c],
            near_recv.at[0, c],
            near,
        )
        for c in range(chunks)
    ]
    on_near = [
        remote(
            downs.at[0, :, cols(c)],
            downs.at[2, :, cols(c)],
            near_send.at[1, c],
            near_recv.at[1, c],
            near,
        )
        for c in range(chunks)
    ]
    crossings = [
        remote(give, arr.at[i], rs_send.at[i], rs_recv.at[i], far)
        for i, give in enumerate((give_s, give_m))
    ]
    for copy in to_far:
        copy.start()
    relay.start()
    for copy in to_near:
        copy.start()
    for copy in crossings:
        copy.start()

    def product(slot):
        acc[...] = jnp.zeros_like(acc)

        @pl.loop(0, rows_ref.shape[1] // DEPTH)
        def _(k):
            part = pl.ds(pl.multiple_of(k * DEPTH, DEPTH), DEPTH)
            acc[...] += jnp.dot(
                rows_ref[:, part], wbuf[slot, part, :], preferred_element_type=jnp.float32
            )

        return acc[...]

    for turn, slot in enumerate((0, 2, 1, 3)):
        if turn < 3:
            loads[2 * turn].wait()
            loads[2 * turn + 1].wait()
        else:
            loads[6].wait()
            relay.wait()
        gate = product(slot)
        gate = gate * jax.nn.sigmoid(gate)
        hid[slot] = (gate * product(slot + 4)).astype(jnp.bfloat16)

    def back(c, j):
        to = lax.rem(me + j, count)
        return remote(
            prod.at[c, to], ret.at[c, me], ret_send.at[c, to], ret_recv.at[c, me], {"ep": to}
        )

    for c in range(chunks):
        to_far[c].wait()
        on_near[c].start()
        to_near[c].wait()

        def partly(at):
            total = jnp.dot(hid[0], down_ref[:, at], preferred_element_type=jnp.float32)
            for piece, slot in ((0, 1), (1, 2)):
                total += jnp.dot(hid[slot], downs[piece, :, at], preferred_element_type=jnp.float32)
            return total

        on_near[c].wait()

        @pl.loop(0, chunk // TILE)
        def _(i):
            at = pl.ds(pl.multiple_of(c * chunk + i * TILE, TILE), TILE)
            total = partly(at)
            total += jnp.dot(hid[3], downs[2, :, at], preferred_element_type=jnp.float32)
            prod[c, :, :, pl.ds(pl.multiple_of(i * TILE, TILE), TILE)] = total.astype(
                jnp.bfloat16
            ).reshape(count, cap, TILE)

        @pl.loop(1, count)
        def _(j):
            back(c, j).start()

        ret[c, me] = prod[c, me]

    crossings[0].wait()
    for c in range(chunks):

        @pl.loop(1, count)
        def _(j):
            source = lax.rem(me + j, count)
            remote(
                prod.at[c, source],
                ret.at[c, source],
                ret_send.at[c, source],
                ret_recv.at[c, source],
                {"ep": source},
            ).wait()

        @pl.loop(0, chunk // TILE)
        def _(i):
            here = pl.ds(pl.multiple_of(i * TILE, TILE), TILE)
            at = pl.ds(pl.multiple_of(c * chunk + i * TILE, TILE), TILE)
            total = (keep_s[:, at] + arr[0, :, at].astype(jnp.float32)).astype(jnp.bfloat16)
            total = total.astype(jnp.float32)
            came = ret[c, :, :, here].reshape(count * cap, TILE)
            for k in range(choice_ref.shape[0]):
                picked = jnp.dot(choice_ref[k], came, preferred_element_type=jnp.float32)
                total += picked * share_ref[:, k : k + 1]
            out_ref[:, at] = total.astype(jnp.bfloat16)

    crossings[1].wait()

    @pl.loop(0, mixer_ref.shape[1] // TILE)
    def _(i):
        at = pl.ds(pl.multiple_of(i * TILE, TILE), TILE)
        mixer_ref[:, at] = (keep_m[:, at] + arr[1, :, at].astype(jnp.float32)).astype(jnp.bfloat16)


def experts_and_rest(rows_in, gates, ups, down, choice, share, give_s, give_m, keep_s, keep_m):
    count = lax.axis_size("ep")
    rows, width = give_s.shape
    slots, hidden = rows_in.shape[0], down.shape[0]
    cap, chunk = slots // count, width // COLUMN_CHUNKS
    far = pl.BlockSpec(memory_space=pl.ANY)
    vmem = pl.BlockSpec(memory_space=pltpu.VMEM)
    bf16, dma = jnp.bfloat16, pltpu.SemaphoreType.DMA
    return pl.pallas_call(
        expert_kernel,
        out_shape=[jax.ShapeDtypeStruct((rows, width), bf16)] * 2,
        in_specs=[vmem] + [far] * 7 + [vmem] * 7,
        out_specs=[vmem, vmem],
        scratch_shapes=[
            pltpu.VMEM((8, width, hidden), bf16),
            pltpu.VMEM((slots, hidden), jnp.float32),
            pltpu.VMEM((4, slots, hidden), bf16),
            pltpu.VMEM((3, hidden, width), bf16),
            pltpu.VMEM((COLUMN_CHUNKS, count, cap, chunk), bf16),
            pltpu.VMEM((COLUMN_CHUNKS, count, cap, chunk), bf16),
            pltpu.VMEM((2, rows, width), bf16),
            dma((8,)),
            dma((2,)),
            dma((COLUMN_CHUNKS,)),
            dma((COLUMN_CHUNKS,)),
            dma((2, COLUMN_CHUNKS)),
            dma((2, COLUMN_CHUNKS)),
            dma((2,)),
            dma((2,)),
            dma((COLUMN_CHUNKS, count)),
            dma((COLUMN_CHUNKS, count)),
        ],
        compiler_params=pltpu.CompilerParams(
            collective_id=0, has_side_effects=True, vmem_limit_bytes=63 * 2**20
        ),
        cost_estimate=pl.CostEstimate(
            flops=6 * slots * width * hidden * 4, bytes_accessed=2**24, transcendentals=0
        ),
    )(rows_in, *gates, *ups, down, choice, share, give_s, give_m, keep_s, keep_m)


def rms_normed(features, gain):
    features = features.astype(jnp.float32)
    return (
        features
        * lax.rsqrt(jnp.mean(features * features, axis=1, keepdims=True) + EPSILON)
        * gain
    ).astype(jnp.bfloat16)


def gated_hidden(rows_in, weight_gate, weight_up):
    return (
        jax.nn.silu(jnp.dot(rows_in, weight_gate, preferred_element_type=jnp.float32))
        * jnp.dot(rows_in, weight_up, preferred_element_type=jnp.float32)
    ).astype(jnp.bfloat16)


def layer(
    value_in,
    gate_in,
    conv_taps,
    conv_bias,
    ln_gain,
    ln_bias,
    out_proj,
    tokens_b,
    norm_gain,
    routes,
    route_weights,
    expert_gate,
    expert_up,
    expert_down,
    shared_gate,
    shared_up,
    shared_down,
):
    tp_count = lax.axis_size("tp")
    ep_count = lax.axis_size("ep")
    model_width = tokens_b.shape[1]
    rows_own, top_count = routes.shape
    capacity = 3 * rows_own * top_count // (2 * ep_count)
    capacity = -(-capacity // 16) * 16

    far_gate = swapped(expert_gate[0], "tp", FAR)
    gates = [expert_gate[0], far_gate]
    gates += [swapped(g, "tp", NEAR) for g in gates]

    own = lax.dynamic_slice_in_dim(tokens_b, lax.axis_index("tp") * rows_own, rows_own, 0)
    own_rows = rms_normed(own, norm_gain)
    by_choice = routes.T
    expert_ids = jnp.arange(ep_count, dtype=jnp.int32)
    names = by_choice[:, None, :] == expert_ids[None, :, None]
    named = jnp.any(names, axis=0)
    row_ids = jnp.arange(rows_own, dtype=jnp.int32)
    before_row = (row_ids[:, None] < row_ids[None, :]).astype(jnp.bfloat16)
    earlier = jnp.dot(
        named.astype(jnp.bfloat16), before_row, preferred_element_type=jnp.float32
    ).astype(jnp.int32)
    slots = jnp.arange(capacity, dtype=jnp.int32)
    placed = earlier[:, None, :] == slots[None, :, None]
    pick = (placed & named[:, None, :]).astype(jnp.bfloat16).reshape(-1, rows_own)
    outbox = jnp.dot(pick, own_rows, preferred_element_type=jnp.float32).astype(jnp.bfloat16)
    arrived = lax.all_to_all(
        outbox.reshape(ep_count, capacity, model_width), "ep", split_axis=0, concat_axis=0, tiled=True
    ).reshape(ep_count * capacity, model_width)

    gated = (value_in.astype(jnp.float32) * jax.nn.sigmoid(gate_in.astype(jnp.float32))).astype(
        jnp.bfloat16
    )
    rim_rows = conv_taps.shape[0] - 1
    length = gated.shape[0]
    before = shifted(gated[length - rim_rows :], "ep", 1)
    padded = jnp.concatenate([before, gated], axis=0).astype(jnp.float32)
    filtered = jnp.zeros(gated.shape, jnp.float32) + conv_bias[None, :]
    for tap_index in range(rim_rows + 1):
        filtered = filtered + conv_taps[tap_index][None, :] * padded[tap_index : tap_index + length]
    sums = jnp.stack([jnp.sum(filtered, axis=1), jnp.sum(filtered * filtered, axis=1)])
    near = sums + swapped(sums, "tp", 1)
    far = swapped(near, "tp", 2)
    wide, near_kept = lax.optimization_barrier((expert_up[0], near))
    far_up = swapped(wide, "tp", FAR)
    ups = [wide, far_up, swapped(wide, "tp", NEAR)]
    row_sum, squares = near_kept + far
    normed_b = rms_normed(tokens_b, norm_gain)
    hidden_shared = gated_hidden(normed_b, shared_gate, shared_up)
    give_s, keep_s = half_scattered(hidden_shared, shared_down)
    channel_count = filtered.shape[1] * tp_count
    average = row_sum / channel_count
    variance = squares / channel_count - average * average
    scale = lax.rsqrt(variance + EPSILON)
    normed_a = (filtered - average[:, None]) * scale[:, None] * ln_gain + ln_bias
    activated = jax.nn.silu(normed_a).astype(jnp.bfloat16)
    give_m, keep_m = half_scattered(activated, out_proj)

    choice = jnp.stack(
        [
            (placed & names[k][:, None, :]).astype(jnp.bfloat16).reshape(-1, rows_own).T
            for k in range(top_count)
        ]
    )
    mixer_rows, outs = experts_and_rest(
        arrived,
        gates,
        ups,
        expert_down[0],
        choice,
        route_weights,
        give_s,
        give_m,
        keep_s,
        keep_m,
    )
    return (mixer_rows, outs)


def solution(mesh):
    return jax.shard_map(
        layer,
        mesh=mesh,
        in_specs=(
            P("ep", "tp"),
            P("ep", "tp"),
            P(None, "tp"),
            P("tp"),
            P("tp"),
            P("tp"),
            P("tp", None),
            P("ep", None),
            P(),
            P(("ep", "tp"), None),
            P(("ep", "tp"), None),
            P("ep", None, "tp"),
            P("ep", None, "tp"),
            P("ep", "tp", None),
            P(None, "tp"),
            P(None, "tp"),
            P("tp", None),
        ),
        out_specs=(P(("ep", "tp"), None), P(("ep", "tp"), None)),
        check_vma=False,
    )
```

```python
import jax
import jax.numpy as jnp
from jax import lax
from jax.experimental import pallas as pl
from jax.experimental.pallas import tpu as pltpu
from jax.sharding import PartitionSpec as P

MESH = pl.DeviceIdType.MESH
EPSILON = 1e-06
CHUNKS = 4
TILE = 256
STEP = 32
RIM = 32
F32, BF16 = jnp.float32, jnp.bfloat16


def dot(a, b):
    return jnp.dot(a, b, preferred_element_type=F32)


def silu(v):
    return v * jax.nn.sigmoid(v)


def aligned(i, size):
    return pl.ds(pl.multiple_of(i * size, size), size)


def kernel(
    value,
    gate,
    taps,
    bias,
    ln_gain,
    ln_bias,
    norm_gain,
    routes,
    share,
    out_proj,
    tokens,
    expert_gate,
    expert_up,
    expert_down,
    shared_gate,
    shared_up,
    shared_down,
    mixer_ref,
    out_ref,
    wbuf,
    opbuf,
    downs,
    tok,
    box,
    rows,
    ret,
    pad,
    act,
    hs,
    ns,
    kept,
    nr,
    arr,
    sacc,
    gacc,
    hid,
    stat,
    cols_st,
    choice,
    load,
    put_sem,
    tok_load,
    halo_sem,
    stat_sem,
    w_send,
    w_recv,
    down_send,
    down_recv,
    near_send,
    near_recv,
    rs_near,
    rs_far,
    go_send,
    go_recv,
    ret_send,
    ret_recv,
):
    me, t = lax.axis_index("ep"), lax.axis_index("tp")
    count = lax.axis_size("ep")
    _, _, cap, chunk = box.shape
    own = share.shape[0]
    length, width = value.shape[0], tok.shape[1]
    slots = count * cap
    core, low = lax.rem(t, 2), t // 2
    near = {"tp": t + 1 - 2 * core}
    far = {"tp": lax.rem(t + 2, 4)}
    hidden = hs.shape[1]

    def remote(src, dst, send, recv, to):
        return pltpu.make_async_remote_copy(
            src_ref=src, dst_ref=dst, send_sem=send, recv_sem=recv, device_id=to, device_id_type=MESH
        )

    def fetch(src, dst, i):
        return pltpu.make_async_copy(src, dst, load.at[i])

    def cols(c):
        return pl.ds(c * chunk, chunk)

    barrier = pltpu.get_barrier_semaphore()
    pl.semaphore_signal(barrier, inc=1, device_id=near, device_id_type=MESH)
    pl.semaphore_signal(barrier, inc=1, device_id=far, device_id_type=MESH)

    @pl.loop(1, count)
    def _(j):
        pl.semaphore_signal(
            barrier, inc=1, device_id={"ep": lax.rem(me + j, count)}, device_id_type=MESH
        )

    def tokens_load(b):
        return pltpu.make_async_copy(tokens.at[aligned(b, own)], tok.at[aligned(b, own)], tok_load.at[b])

    tokens_load(t).start()
    get_sg = fetch(shared_gate, wbuf.at[0], 0)
    get_su = fetch(shared_up, wbuf.at[4], 1)
    get_sd = fetch(shared_down, opbuf.at[pl.ds(0, hidden)], 2)
    get_sg.start()
    get_su.start()
    get_sd.start()

    @pl.loop(1, 4)
    def _(j):
        tokens_load(lax.rem(t + j, 4)).start()

    pl.semaphore_wait(barrier, count + 1)

    gate_far = remote(expert_gate, wbuf.at[1], w_send.at[0], w_recv.at[0], far)
    gate_near = remote(expert_gate, wbuf.at[2], w_send.at[1], w_recv.at[1], near)
    gate_on = remote(wbuf.at[1], wbuf.at[3], w_send.at[2], w_recv.at[2], near)
    up_far = remote(expert_up, wbuf.at[5], w_send.at[3], w_recv.at[3], far)
    up_near = remote(expert_up, wbuf.at[6], w_send.at[4], w_recv.at[4], near)
    up_on = remote(wbuf.at[5], wbuf.at[7], w_send.at[5], w_recv.at[5], near)
    down_far = [
        remote(expert_down.at[:, cols(c)], downs.at[0, :, cols(c)], down_send.at[c], down_recv.at[c], far)
        for c in range(CHUNKS)
    ]
    down_near = [
        remote(
            expert_down.at[:, cols(c)],
            downs.at[1, :, cols(c)],
            near_send.at[0, c],
            near_recv.at[0, c],
            near,
        )
        for c in range(CHUNKS)
    ]
    down_on = [
        remote(
            downs.at[0, :, cols(c)],
            downs.at[2, :, cols(c)],
            near_send.at[1, c],
            near_recv.at[1, c],
            near,
        )
        for c in range(CHUNKS)
    ]
    gate_far.start()
    gate_near.start()

    @pl.loop(0, length // STEP)
    def _(i):
        at = aligned(i, STEP)
        gated = value[at, :].astype(F32) * jax.nn.sigmoid(gate[at, :].astype(F32))
        pad[aligned(i + 1, STEP), :] = gated.astype(BF16).astype(F32)

    def halo(to):
        return remote(
            pad.at[pl.ds(length, RIM)], pad.at[pl.ds(0, RIM)], halo_sem.at[0], halo_sem.at[1], {"ep": to}
        )

    @pl.when(me < count - 1)
    def _():
        halo(lax.rem(me + 1, count)).start()

    @pl.when(me == 0)
    def _():
        pad[pl.ds(0, RIM), :] = jnp.zeros((RIM, pad.shape[1]), F32)

    def normalize(b):
        tokens_load(b).wait()

        @pl.loop(0, own // 16)
        def _(i):
            at = pl.ds(pl.multiple_of(b * own + i * 16, 16), 16)
            x = tok[at, :].astype(F32)
            scale = lax.rsqrt(jnp.mean(x * x, axis=1, keepdims=True) + EPSILON)
            tok[at, :] = (x * scale * norm_gain[...]).astype(BF16)

    normalize(t)
    lanes = lax.broadcasted_iota(jnp.int32, (own, 128), 1)
    names = [(lanes == routes[:, k : k + 1]).astype(F32) for k in range(routes.shape[1])]
    before = lax.broadcasted_iota(jnp.int32, (own, own), 1) < lax.broadcasted_iota(
        jnp.int32, (own, own), 0
    )
    earlier = dot(before.astype(F32).astype(BF16), sum(names).astype(BF16))
    places = lax.broadcasted_iota(jnp.int32, (own, slots), 1).astype(F32)
    anywhere = jnp.zeros((own, slots), F32)
    for k, name in enumerate(names):
        place = jnp.sum(earlier * name, axis=1, keepdims=True)
        place = place + routes[:, k : k + 1].astype(F32) * cap
        chosen = (places == place).astype(F32)
        anywhere = anywhere + chosen
        choice[k] = chosen.astype(BF16)
    pick = anywhere.T.astype(BF16)

    def going(c, j):
        to = lax.rem(me + j, count)
        return remote(box.at[c, to], rows.at[c, me], go_send.at[c, to], go_recv.at[c, me], {"ep": to})

    for c in range(CHUNKS):

        @pl.loop(0, chunk // TILE)
        def _(i):
            at = pl.ds(pl.multiple_of(c * chunk + i * TILE, TILE), TILE)
            sent = dot(pick, tok[aligned(t, own), at]).astype(BF16)
            box[c, :, :, aligned(i, TILE)] = sent.reshape(count, cap, TILE)

        @pl.loop(1, count)
        def _(j):
            going(c, j).start()

        rows[c, me] = box[c, me]

    @pl.when(me < count - 1)
    def _():
        halo(lax.rem(me + 1, count)).wait_send()

    @pl.when(me > 0)
    def _():
        halo(lax.rem(me + 1, count)).wait_recv()

    tap_count = taps.shape[0]
    first = RIM - (tap_count - 1)

    @pl.loop(0, length // STEP)
    def _(i):
        window = pad[pl.ds(pl.multiple_of(i * STEP, STEP), STEP + RIM), :]
        total = jnp.zeros((STEP, window.shape[1]), F32) + bias[...]
        for s in range(8):
            turned = pltpu.roll(window, STEP + RIM - s, 0) if s else window
            for q in range((RIM + 8) // 8):
                j = s + 8 * q - first
                if 0 <= j < tap_count:
                    total = total + taps[j : j + 1, :] * turned[8 * q : 8 * q + STEP]
        pad[aligned(i, STEP), :] = total
        lane = lax.broadcasted_iota(jnp.int32, (STEP, 128), 1)
        plain = jnp.sum(total, axis=1, keepdims=True)
        square = jnp.sum(total * total, axis=1, keepdims=True)
        cols_st[aligned(i, STEP), :] = jnp.where(
            lane == 0, plain, jnp.where(lane == 1, square, 0.0)
        )

    stat[0] = cols_st[...].T[:8]
    stat_near = remote(stat.at[0], stat.at[1], stat_sem.at[0], stat_sem.at[1], near)
    stat_near.start()
    stat_near.wait()
    stat[2] = stat[0] + stat[1]
    stat_far = remote(stat.at[2], stat.at[3], stat_sem.at[2], stat_sem.at[3], far)
    stat_far.start()
    up_far.start()
    for c in range(CHUNKS):
        down_far[c].start()
    up_near.start()
    for c in range(CHUNKS):
        down_near[c].start()

    @pl.loop(1, 4)
    def _(j):
        normalize(lax.rem(t + j, 4))

    get_sg.wait()
    get_su.wait()
    sacc[...] = jnp.zeros_like(sacc)

    @pl.loop(0, CHUNKS)
    def _(k):
        at = aligned(k, chunk)
        sacc[0] += dot(tok[:, at], wbuf[0, at, :])
        sacc[1] += dot(tok[:, at], wbuf[4, at, :])

    get_own_gate = fetch(expert_gate, wbuf.at[0], 3)
    get_own_up = fetch(expert_up, wbuf.at[4], 4)
    get_own_gate.start()
    get_own_up.start()
    hs[...] = (silu(sacc[0]) * sacc[1]).astype(BF16)

    def halves(which, lhs, depth):
        @pl.loop(0, width // TILE)
        def _(i):
            at = aligned(i, TILE)
            for j in range(2):
                block = aligned(2 * j + 1 - core, own)
                ns[j, :, at] = dot(lhs[block, :], opbuf[pl.ds(0, depth), at]).astype(BF16)
            for j in range(2):
                block = aligned(2 * j + core, own)
                kept[which, j, :, at] = dot(lhs[block, :], opbuf[pl.ds(0, depth), at]).astype(BF16)

    to_near = [
        remote(ns, nr.at[which], rs_near.at[which, 0], rs_near.at[which, 1], near) for which in range(2)
    ]
    crossing = [
        remote(kept.at[which, 1 - low], arr.at[which], rs_far.at[which, 0], rs_far.at[which, 1], far)
        for which in range(2)
    ]

    def cross(which):
        to_near[which].wait_recv()

        @pl.loop(0, own // 16)
        def _(i):
            at = aligned(i, 16)
            kept[which, 1 - low, at, :] = (
                kept[which, 1 - low, at, :].astype(F32) + nr[which, 1 - low, at, :].astype(F32)
            ).astype(BF16)

        crossing[which].start()

    get_sd.wait()
    halves(0, hs, hidden)
    to_near[0].start()
    get_op = fetch(out_proj, opbuf, 5)
    get_op.start()

    stat_far.wait()
    cross(0)
    total = stat[2] + stat[3]
    cols_st[...] = jnp.concatenate([total, jnp.zeros((120, length), F32)], axis=0).T
    channels = pad.shape[1] * 4

    @pl.loop(0, length // STEP)
    def _(i):
        at = aligned(i, STEP)
        average = cols_st[at, 0:1] / channels
        variance = cols_st[at, 1:2] / channels - average * average
        scale = lax.rsqrt(variance + EPSILON)
        v = (pad[at, :] - average) * scale * ln_gain[...] + ln_bias[...]
        act[at, :] = silu(v).astype(BF16)

    gate_far.wait()
    gate_on.start()
    get_op.wait()
    to_near[0].wait_send()
    halves(1, act, act.shape[1])
    to_near[1].start()
    get_down = fetch(expert_down, opbuf.at[pl.ds(0, hidden)], 6)
    get_down.start()
    cross(1)

    for c in range(CHUNKS):

        @pl.loop(1, count)
        def _(j):
            source = lax.rem(me + j, count)
            remote(
                box.at[c, source],
                rows.at[c, source],
                go_send.at[c, source],
                go_recv.at[c, source],
                {"ep": source},
            ).wait()

    def product(into, slot):
        into[...] = jnp.zeros(into.shape, F32)

        @pl.loop(0, CHUNKS)
        def _(k):
            into[...] += dot(rows[k].reshape(slots, chunk), wbuf[slot, aligned(k, chunk), :])

    def finish(piece):
        product(sacc.at[0, pl.ds(0, slots)], piece + 4)
        hid[piece] = (silu(gacc[piece]) * sacc[0, pl.ds(0, slots), :]).astype(BF16)

    get_own_gate.wait()
    product(gacc.at[0], 0)
    gate_near.wait()
    product(gacc.at[2], 2)
    product(gacc.at[1], 1)
    gate_on.wait()
    product(gacc.at[3], 3)
    get_own_up.wait()
    finish(0)
    up_near.wait()
    finish(2)
    up_far.wait()
    up_on.start()
    finish(1)
    up_on.wait()
    finish(3)
    get_down.wait()

    def back(c, j):
        to = lax.rem(me + j, count)
        return remote(box.at[c, to], ret.at[c, me], ret_send.at[c, to], ret_recv.at[c, me], {"ep": to})

    for c in range(CHUNKS):
        down_far[c].wait()
        down_on[c].start()
        down_near[c].wait()
        down_on[c].wait()

        @pl.loop(0, chunk // TILE)
        def _(i):
            at = pl.ds(pl.multiple_of(c * chunk + i * TILE, TILE), TILE)
            total = dot(hid[0], opbuf[pl.ds(0, hidden), at])
            for piece in range(3):
                total += dot(hid[piece + 1], downs[piece, :, at])
            box[c, :, :, aligned(i, TILE)] = total.astype(BF16).reshape(count, cap, TILE)

        @pl.loop(1, count)
        def _(j):
            back(c, j).start()

        ret[c, me] = box[c, me]

    def ended(which, at):
        return (
            kept[which, low, :, at].astype(F32)
            + nr[which, low, :, at].astype(F32)
            + arr[which, :, at].astype(F32)
        ).astype(BF16)

    def put(which, at, into, i):
        return pltpu.make_async_copy(arr.at[which, :, at], into.at[:, at], put_sem.at[i])

    crossing[0].wait()
    for c in range(CHUNKS):

        @pl.loop(1, count)
        def _(j):
            source = lax.rem(me + j, count)
            remote(
                box.at[c, source],
                ret.at[c, source],
                ret_send.at[c, source],
                ret_recv.at[c, source],
                {"ep": source},
            ).wait()

        @pl.loop(0, chunk // TILE)
        def _(i):
            at = pl.ds(pl.multiple_of(c * chunk + i * TILE, TILE), TILE)
            total = ended(0, at).astype(F32)
            came = ret[c, :, :, aligned(i, TILE)].reshape(slots, TILE)
            for k in range(choice.shape[0]):
                total += dot(choice[k], came) * share[:, k : k + 1]
            arr[0, :, at] = total.astype(BF16)

        put(0, cols(c), out_ref, c).start()

    to_near[1].wait_send()
    crossing[1].wait()

    @pl.loop(0, width // TILE)
    def _(i):
        at = aligned(i, TILE)
        arr[1, :, at] = ended(1, at)

    put(1, pl.ds(0, width), mixer_ref, CHUNKS).start()
    for c in range(CHUNKS):
        put(0, cols(c), out_ref, c).wait()
    put(1, pl.ds(0, width), mixer_ref, CHUNKS).wait()


def per_device(
    value_in,
    gate_in,
    conv_taps,
    conv_bias,
    ln_gain,
    ln_bias,
    out_proj,
    tokens_b,
    norm_gain,
    routes,
    route_weights,
    expert_gate,
    expert_up,
    expert_down,
    shared_gate,
    shared_up,
    shared_down,
):
    ep_count = lax.axis_size("ep")
    own, top_count = routes.shape
    length, channels = value_in.shape
    width, hidden = tokens_b.shape[1], expert_down.shape[1]
    cap = 3 * own * top_count // (2 * ep_count)
    cap = -(-cap // 16) * 16
    slots, chunk = ep_count * cap, width // CHUNKS
    anywhere = pl.BlockSpec(memory_space=pl.ANY)
    vmem = pl.BlockSpec(memory_space=pltpu.VMEM)
    dma = pltpu.SemaphoreType.DMA
    mail = pltpu.VMEM((CHUNKS, ep_count, cap, chunk), BF16)
    return pl.pallas_call(
        kernel,
        out_shape=[jax.ShapeDtypeStruct((own, width), BF16)] * 2,
        in_specs=[vmem] * 9 + [anywhere] * 8,
        out_specs=[anywhere, anywhere],
        scratch_shapes=[
            pltpu.VMEM((8, width, hidden), BF16),
            pltpu.VMEM((max(channels, hidden), width), BF16),
            pltpu.VMEM((3, hidden, width), BF16),
            pltpu.VMEM((4 * own, width), BF16),
            mail,
            mail,
            mail,
            pltpu.VMEM((length + RIM, channels), F32),
            pltpu.VMEM((length, channels), BF16),
            pltpu.VMEM((4 * own, hidden), BF16),
            pltpu.VMEM((2, own, width), BF16),
            pltpu.VMEM((2, 2, own, width), BF16),
            pltpu.VMEM((2, 2, own, width), BF16),
            pltpu.VMEM((2, own, width), BF16),
            pltpu.VMEM((2, 4 * own, hidden), F32),
            pltpu.VMEM((4, slots, hidden), F32),
            pltpu.VMEM((4, slots, hidden), BF16),
            pltpu.VMEM((4, 8, length), F32),
            pltpu.VMEM((length, 128), F32),
            pltpu.VMEM((top_count, own, slots), BF16),
            dma((7,)),
            dma((CHUNKS + 1,)),
            dma((4,)),
            dma((2,)),
            dma((4,)),
            dma((6,)),
            dma((6,)),
            dma((CHUNKS,)),
            dma((CHUNKS,)),
            dma((2, CHUNKS)),
            dma((2, CHUNKS)),
            dma((2, 2)),
            dma((2, 2)),
            dma((CHUNKS, ep_count)),
            dma((CHUNKS, ep_count)),
            dma((CHUNKS, ep_count)),
            dma((CHUNKS, ep_count)),
        ],
        compiler_params=pltpu.CompilerParams(
            collective_id=0, has_side_effects=True, vmem_limit_bytes=67043328
        ),
    )(
        value_in,
        gate_in,
        conv_taps,
        conv_bias[None],
        ln_gain[None],
        ln_bias[None],
        norm_gain[None],
        routes,
        route_weights,
        out_proj,
        tokens_b,
        expert_gate[0],
        expert_up[0],
        expert_down[0],
        shared_gate,
        shared_up,
        shared_down,
    )


def solution(mesh):
    return jax.shard_map(
        lambda *args: tuple(per_device(*args)),
        mesh=mesh,
        in_specs=(
            P("ep", "tp"),
            P("ep", "tp"),
            P(None, "tp"),
            P("tp"),
            P("tp"),
            P("tp"),
            P("tp", None),
            P("ep", None),
            P(),
            P(("ep", "tp"), None),
            P(("ep", "tp"), None),
            P("ep", None, "tp"),
            P("ep", None, "tp"),
            P("ep", "tp", None),
            P(None, "tp"),
            P(None, "tp"),
            P("tp", None),
        ),
        out_specs=(P(("ep", "tp"), None), P(("ep", "tp"), None)),
        check_vma=False,
    )
```

```python
import jax
import jax.numpy as jnp
from jax import lax
from jax.experimental import pallas as pl
from jax.experimental.pallas import tpu as pltpu
from jax.sharding import PartitionSpec as P

MESH = pl.DeviceIdType.MESH
EPSILON = 1e-06
CHUNKS = 4
TILE = 256
STEP = 32
UNIT = 16
RIM = 32
F32, BF16 = jnp.float32, jnp.bfloat16


def dot(a, b):
    return jnp.dot(a, b, preferred_element_type=F32)


def silu(v):
    return v * jax.nn.sigmoid(v)


def aligned(i, size):
    return pl.ds(pl.multiple_of(i * size, size), size)


def kernel(
    value,
    gate,
    taps,
    bias,
    ln_gain,
    ln_bias,
    norm_gain,
    routes,
    share,
    out_proj,
    tokens,
    expert_gate,
    expert_up,
    expert_down,
    shared_gate,
    shared_up,
    shared_down,
    mixer_ref,
    out_ref,
    wbuf,
    opbuf,
    dbuf,
    downs,
    tok,
    box,
    dup,
    rows,
    frows,
    ret,
    pad,
    act,
    hs,
    ns,
    kept,
    nr,
    arr,
    sacc,
    hid,
    hfar,
    total_out,
    stat,
    cols_st,
    choice,
    share_cols,
    froutes,
    load,
    put_sem,
    tok_load,
    halo_sem,
    stat_sem,
    route_sem,
    w_send,
    w_recv,
    down_send,
    down_recv,
    near_send,
    near_recv,
    rs_near,
    rs_far,
    go_send,
    go_recv,
    dup_send,
    dup_recv,
    f_send,
    f_recv,
    h_send,
    h_recv,
    ret_send,
    ret_recv,
):
    me, t = lax.axis_index("ep"), lax.axis_index("tp")
    count = lax.axis_size("ep")
    groups = box.shape[0]
    own = share.shape[1]
    length, width = value.shape[0], tok.shape[1]
    chunk = width // CHUNKS
    batch = count * UNIT
    core, low = lax.rem(t, 2), t // 2
    near = {"tp": t + 1 - 2 * core}
    far = {"tp": lax.rem(t + 2, 4)}
    far_t = lax.rem(t + 2, 4)
    base = (me // 2) * 2
    partner = base + 1 - lax.rem(me, 2)
    hidden = hs.shape[1]
    tiles = width // TILE

    def remote(src, dst, send, recv, to):
        return pltpu.make_async_remote_copy(
            src_ref=src, dst_ref=dst, send_sem=send, recv_sem=recv, device_id=to, device_id_type=MESH
        )

    def fetch(src, dst, i):
        return pltpu.make_async_copy(src, dst, load.at[i])

    def cols(c):
        return pl.ds(c * chunk, chunk)

    barrier = pltpu.get_barrier_semaphore()
    pl.semaphore_signal(barrier, inc=1, device_id=near, device_id_type=MESH)
    pl.semaphore_signal(barrier, inc=1, device_id=far, device_id_type=MESH)

    @pl.loop(1, count)
    def _(j):
        pl.semaphore_signal(
            barrier, inc=1, device_id={"ep": lax.rem(me + j, count)}, device_id_type=MESH
        )

    def tokens_load(b):
        return pltpu.make_async_copy(tokens.at[aligned(b, own)], tok.at[aligned(b, own)], tok_load.at[b])

    tokens_load(t).start()
    tokens_load(far_t).start()
    get_sg = fetch(shared_gate, wbuf.at[0], 0)
    get_su = fetch(shared_up, wbuf.at[2], 1)
    get_sd = fetch(shared_down, opbuf.at[pl.ds(0, hidden)], 2)
    get_down = fetch(expert_down, dbuf, 6)
    get_sg.start()
    get_su.start()
    tokens_load(lax.rem(t + 1, 4)).start()
    tokens_load(lax.rem(t + 3, 4)).start()
    get_sd.start()
    get_down.start()
    pl.semaphore_wait(barrier, count + 1)

    routes_far = remote(routes, froutes, route_sem.at[0], route_sem.at[1], far)
    gate_near = remote(expert_gate, wbuf.at[1], w_send.at[0], w_recv.at[0], near)
    up_near = remote(expert_up, wbuf.at[3], w_send.at[1], w_recv.at[1], near)
    down_far = [
        remote(expert_down.at[:, cols(c)], downs.at[0, :, cols(c)], down_send.at[c], down_recv.at[c], far)
        for c in range(CHUNKS)
    ]
    down_near = [
        remote(
            expert_down.at[:, cols(c)],
            downs.at[1, :, cols(c)],
            near_send.at[0, c],
            near_recv.at[0, c],
            near,
        )
        for c in range(CHUNKS)
    ]
    down_on = [
        remote(
            downs.at[0, :, cols(c)],
            downs.at[2, :, cols(c)],
            near_send.at[1, c],
            near_recv.at[1, c],
            near,
        )
        for c in range(CHUNKS)
    ]
    routes_far.start()
    down_far[0].start()
    down_far[1].start()
    gate_near.start()
    up_near.start()
    for c in range(CHUNKS):
        down_near[c].start()

    @pl.loop(0, length // STEP)
    def _(i):
        at = aligned(i, STEP)
        gated = value[at, :].astype(F32) * jax.nn.sigmoid(gate[at, :].astype(F32))
        pad[aligned(i + 1, STEP), :] = gated.astype(BF16).astype(F32)

    def halo(to):
        return remote(
            pad.at[pl.ds(length, RIM)], pad.at[pl.ds(0, RIM)], halo_sem.at[0], halo_sem.at[1], {"ep": to}
        )

    @pl.when(me < count - 1)
    def _():
        halo(lax.rem(me + 1, count)).start()

    @pl.when(me == 0)
    def _():
        pad[pl.ds(0, RIM), :] = jnp.zeros((RIM, pad.shape[1]), F32)

    def normalize(b):
        tokens_load(b).wait()

        @pl.loop(0, own // 16)
        def _(i):
            at = pl.ds(pl.multiple_of(b * own + i * 16, 16), 16)
            x = tok[at, :].astype(F32)
            scale = lax.rsqrt(jnp.mean(x * x, axis=1, keepdims=True) + EPSILON)
            tok[at, :] = (x * scale * norm_gain[...]).astype(BF16)

    def tall(wide):
        return jnp.concatenate([wide, jnp.zeros((own - wide.shape[0], own), F32)], axis=0).T

    def placed(ids):
        lanes = lax.broadcasted_iota(jnp.int32, (own, own), 1).astype(F32)
        columns = tall(ids.astype(F32))
        chosen = [columns[:, k : k + 1] for k in range(ids.shape[0])]
        names = [(lanes == r).astype(F32) for r in chosen]
        before = lax.broadcasted_iota(jnp.int32, (own, own), 1) < lax.broadcasted_iota(
            jnp.int32, (own, own), 0
        )
        earlier = dot(before.astype(F32).astype(BF16), sum(names).astype(BF16))
        return [
            (r, jnp.sum(earlier * name, axis=1, keepdims=True)) for r, name in zip(chosen, names)
        ]

    normalize(t)
    share_cols[...] = tall(share[...])
    places = lax.broadcasted_iota(jnp.int32, (own, groups * batch), 1).astype(F32)
    anywhere = jnp.zeros((own, groups * batch), F32)
    for k, (r, place) in enumerate(placed(routes[...])):
        spot = place + UNIT * (r + (count - 1) * jnp.floor(place * (1 / UNIT)))
        chosen = (places == spot).astype(F32)
        anywhere = anywhere + chosen
        for g in range(groups):
            choice[k, g] = chosen[:, g * batch : (g + 1) * batch].astype(BF16)
    pick = anywhere.T.astype(BF16)

    def going(g, to):
        return remote(box.at[g, to], rows.at[g, me], go_send.at[g, to], go_recv.at[g, me], {"ep": to})

    def came(g, source):
        return remote(
            box.at[g, source], rows.at[g, source], go_send.at[g, source], go_recv.at[g, source], {"ep": source}
        )

    for g in range(groups):
        part = pick[g * batch : (g + 1) * batch]

        @pl.loop(0, tiles)
        def _(i):
            at = aligned(i, TILE)
            box[g, :, :, at] = dot(part, tok[aligned(t, own), at]).astype(BF16).reshape(count, UNIT, TILE)

        @pl.loop(1, count)
        def _(j):
            going(g, lax.rem(me + j, count)).start()

        rows[g, me] = box[g, me]

    normalize(far_t)
    routes_far.wait()
    spots = lax.broadcasted_iota(jnp.int32, (own, own), 1).astype(F32)
    anywhere = jnp.zeros((own, own), F32)
    first_of_pair = base.astype(F32)
    for r, place in placed(froutes[...]):
        inside = (r - first_of_pair >= 0) & (r - first_of_pair <= 1)
        spot = place + UNIT * (r - first_of_pair + jnp.floor(place * (1 / UNIT)))
        anywhere = anywhere + jnp.where(inside & (spots == spot), 1.0, 0.0)
    pick = anywhere.T.astype(BF16)[: groups * 2 * UNIT]

    @pl.loop(0, tiles)
    def _(i):
        at = aligned(i, TILE)
        dup[:, :, :, at] = (
            dot(pick, tok[aligned(far_t, own), at]).astype(BF16).reshape(groups, 2, UNIT, TILE)
        )

    doubles = [
        remote(
            dup.at[g, partner - base], frows.at[g, me], dup_send.at[g], dup_recv.at[g], {"ep": partner}
        )
        for g in range(groups)
    ]
    for g in range(groups):
        doubles[g].start()
        frows[g, me] = dup[g, me - base]

    @pl.when(me < count - 1)
    def _():
        halo(lax.rem(me + 1, count)).wait_send()

    @pl.when(me > 0)
    def _():
        halo(lax.rem(me + 1, count)).wait_recv()

    tap_count = taps.shape[0]
    first = RIM - (tap_count - 1)

    @pl.loop(0, length // STEP)
    def _(i):
        window = pad[pl.ds(pl.multiple_of(i * STEP, STEP), STEP + RIM), :]
        total = jnp.zeros((STEP, window.shape[1]), F32) + bias[...]
        for s in range(8):
            turned = pltpu.roll(window, STEP + RIM - s, 0) if s else window
            for q in range((RIM + 8) // 8):
                j = s + 8 * q - first
                if 0 <= j < tap_count:
                    total = total + taps[j : j + 1, :] * turned[8 * q : 8 * q + STEP]
        pad[aligned(i, STEP), :] = total
        lane = lax.broadcasted_iota(jnp.int32, (STEP, 128), 1)
        plain = jnp.sum(total, axis=1, keepdims=True)
        square = jnp.sum(total * total, axis=1, keepdims=True)
        cols_st[aligned(i, STEP), :] = jnp.where(
            lane == 0, plain, jnp.where(lane == 1, square, 0.0)
        )

    stat[0] = cols_st[...].T[:8]
    stat_near = remote(stat.at[0], stat.at[1], stat_sem.at[0], stat_sem.at[1], near)
    stat_near.start()

    normalize(lax.rem(t + 1, 4))
    normalize(lax.rem(t + 3, 4))
    stat_near.wait()
    stat[2] = stat[0] + stat[1]
    stat_far = remote(stat.at[2], stat.at[3], stat_sem.at[2], stat_sem.at[3], far)
    stat_far.start()
    get_sg.wait()
    get_su.wait()
    sacc[...] = jnp.zeros_like(sacc)

    @pl.loop(0, CHUNKS)
    def _(k):
        at = aligned(k, chunk)
        sacc[0] += dot(tok[:, at], wbuf[0, at, :])
        sacc[1] += dot(tok[:, at], wbuf[2, at, :])

    get_own_gate = fetch(expert_gate, wbuf.at[0], 3)
    get_own_up = fetch(expert_up, wbuf.at[2], 4)
    get_own_gate.start()
    get_own_up.start()
    hs[...] = (silu(sacc[0]) * sacc[1]).astype(BF16)

    def outside(j):
        return lax.rem(base + 2 + j, count)

    def forward(g, source):
        return remote(
            rows.at[g, source], frows.at[g, source], f_send.at[g, source], f_recv.at[g, source], far
        )

    def forward_group(g):
        @pl.loop(0, count - 2)
        def _(j):
            came(g, outside(j)).wait_recv()
            forward(g, outside(j)).start()

        came(g, partner).wait_recv()

    def far_ready(g):
        doubles[g].wait_recv()

        @pl.loop(0, count - 2)
        def _(j):
            forward(g, outside(j)).wait()

    def ffn(source, g, slot):
        lhs = source.at[g]
        gate_sum = jnp.zeros((batch, hidden), F32)
        up_sum = jnp.zeros((batch, hidden), F32)

        def step(k, sums):
            at = aligned(k, chunk)
            x = lhs[:, :, at].reshape(batch, chunk)
            return sums[0] + dot(x, wbuf[slot, at, :]), sums[1] + dot(x, wbuf[slot + 2, at, :])

        gate_sum, up_sum = lax.fori_loop(0, CHUNKS, step, (gate_sum, up_sum))
        return (silu(gate_sum) * up_sum).astype(BF16)

    def own_part(g):
        hid[g, 0] = ffn(rows, g, 0)
        hid[g, 2] = ffn(rows, g, 1)

    hidden_far = [
        [
            remote(hfar.at[g, n], hid.at[g, 1 + 2 * n], h_send.at[g, n], h_recv.at[g, n], far)
            for n in range(2)
        ]
        for g in range(groups)
    ]

    def far_part(g):
        far_ready(g)
        for n in range(2):
            hfar[g, n] = ffn(frows, g, n)
            hidden_far[g][n].start()

    def halves(which, lhs, depth):
        @pl.loop(0, tiles)
        def _(i):
            at = aligned(i, TILE)
            for j in range(2):
                block = aligned(2 * j + 1 - core, own)
                ns[j, :, at] = dot(lhs[block, :], opbuf[pl.ds(0, depth), at]).astype(BF16)
            for j in range(2):
                block = aligned(2 * j + core, own)
                kept[which, j, :, at] = dot(lhs[block, :], opbuf[pl.ds(0, depth), at]).astype(BF16)

    to_near = [
        remote(ns, nr.at[which], rs_near.at[which, 0], rs_near.at[which, 1], near) for which in range(2)
    ]
    crossing = [
        remote(kept.at[which, 1 - low], arr.at[which], rs_far.at[which, 0], rs_far.at[which, 1], far)
        for which in range(2)
    ]

    def joined(which):
        to_near[which].wait_recv()

        @pl.loop(0, own // 16)
        def _(i):
            at = aligned(i, 16)
            kept[which, 1 - low, at, :] = (
                kept[which, 1 - low, at, :].astype(F32) + nr[which, 1 - low, at, :].astype(F32)
            ).astype(BF16)

    def back(g, to):
        return remote(box.at[g, to], ret.at[g, me], ret_send.at[g, to], ret_recv.at[g, me], {"ep": to})

    def products(g):
        @pl.loop(1, count)
        def _(j):
            came(g, lax.rem(me + j, count)).wait_send()

        for n in range(2):
            hidden_far[g][n].wait()

        @pl.loop(0, tiles)
        def _(i):
            at = aligned(i, TILE)
            total = dot(hid[g, 0], dbuf[:, at])
            for piece in range(3):
                total += dot(hid[g, piece + 1], downs[piece, :, at])
            box[g, :, :, at] = total.astype(BF16).reshape(count, UNIT, TILE)

        @pl.loop(1, count)
        def _(j):
            back(g, lax.rem(me + j, count)).start()

        ret[g, me] = box[g, me]

    def combine(g):
        @pl.loop(1, count)
        def _(j):
            source = lax.rem(me + j, count)
            remote(
                box.at[g, source],
                ret.at[g, source],
                ret_send.at[g, source],
                ret_recv.at[g, source],
                {"ep": source},
            ).wait()

        @pl.loop(0, tiles)
        def _(i):
            at = aligned(i, TILE)
            back_rows = ret[g, :, :, at].reshape(batch, TILE)
            total = jnp.zeros((own, TILE), F32)
            for k in range(choice.shape[0]):
                total += dot(choice[k, g], back_rows) * share_cols[:, k : k + 1]
            if g:
                total += total_out[:, at]
            if g == groups - 1:
                arr[0, :, at] = (total + ended(0, at).astype(F32)).astype(BF16)
            else:
                total_out[:, at] = total

    def ended(which, at):
        return (
            kept[which, low, :, at].astype(F32)
            + nr[which, low, :, at].astype(F32)
            + arr[which, :, at].astype(F32)
        ).astype(BF16)

    def put(which, into):
        return pltpu.make_async_copy(arr.at[which], into, put_sem.at[which])

    def normed():
        stat_far.wait()
        total = stat[2] + stat[3]
        cols_st[...] = jnp.concatenate([total, jnp.zeros((120, length), F32)], axis=0).T
        channels = pad.shape[1] * 4

        @pl.loop(0, length // STEP)
        def _(i):
            at = aligned(i, STEP)
            average = cols_st[at, 0:1] / channels
            variance = cols_st[at, 1:2] / channels - average * average
            scale = lax.rsqrt(variance + EPSILON)
            v = (pad[at, :] - average) * scale * ln_gain[...] + ln_bias[...]
            act[at, :] = silu(v).astype(BF16)

    def relay(c):
        down_far[c].wait()
        down_on[c].start()

    get_op = fetch(out_proj, opbuf, 5)

    forward_group(0)
    down_far[2].start()
    down_far[3].start()
    relay(0)
    relay(1)
    get_own_gate.wait()
    get_own_up.wait()
    gate_near.wait()
    up_near.wait()
    own_part(0)
    get_sd.wait()
    halves(0, hs, hidden)
    to_near[0].start()
    get_op.start()
    far_part(0)
    normed()
    if groups > 1:
        forward_group(1)
        own_part(1)
    get_op.wait()
    to_near[0].wait_send()
    halves(1, act, act.shape[1])
    to_near[1].start()
    joined(0)
    relay(2)
    relay(3)
    get_down.wait()
    for c in range(CHUNKS):
        down_near[c].wait()
        down_on[c].wait()
    products(0)
    for g in range(1, groups):
        if g > 1:
            forward_group(g)
            own_part(g)
    joined(1)
    for g in range(1, groups):
        far_part(g)
    crossing[0].start()
    crossing[1].start()
    for g in range(1, groups):
        products(g)
    for g in range(groups - 1):
        combine(g)
    for g in range(groups):
        doubles[g].wait_send()
    to_near[1].wait_send()
    crossing[0].wait()
    combine(groups - 1)
    put(0, out_ref).start()
    crossing[1].wait()

    @pl.loop(0, tiles)
    def _(i):
        at = aligned(i, TILE)
        arr[1, :, at] = ended(1, at)

    put(1, mixer_ref).start()
    put(0, out_ref).wait()
    put(1, mixer_ref).wait()


def per_device(
    value_in,
    gate_in,
    conv_taps,
    conv_bias,
    ln_gain,
    ln_bias,
    out_proj,
    tokens_b,
    norm_gain,
    routes,
    route_weights,
    expert_gate,
    expert_up,
    expert_down,
    shared_gate,
    shared_up,
    shared_down,
):
    ep_count = lax.axis_size("ep")
    own, top_count = routes.shape
    length, channels = value_in.shape
    width, hidden = tokens_b.shape[1], expert_down.shape[1]
    cap = 3 * own * top_count // (2 * ep_count)
    groups = -(-cap // UNIT)
    batch = ep_count * UNIT
    anywhere = pl.BlockSpec(memory_space=pl.ANY)
    vmem = pl.BlockSpec(memory_space=pltpu.VMEM)
    dma = pltpu.SemaphoreType.DMA
    mail = pltpu.VMEM((groups, ep_count, UNIT, width), BF16)
    return pl.pallas_call(
        kernel,
        out_shape=[jax.ShapeDtypeStruct((own, width), BF16)] * 2,
        in_specs=[vmem] * 9 + [anywhere] * 8,
        out_specs=[anywhere, anywhere],
        scratch_shapes=[
            pltpu.VMEM((4, width, hidden), BF16),
            pltpu.VMEM((max(channels, hidden), width), BF16),
            pltpu.VMEM((hidden, width), BF16),
            pltpu.VMEM((3, hidden, width), BF16),
            pltpu.VMEM((4 * own, width), BF16),
            mail,
            pltpu.VMEM((groups, 2, UNIT, width), BF16),
            mail,
            mail,
            mail,
            pltpu.VMEM((length + RIM, channels), F32),
            pltpu.VMEM((length, channels), BF16),
            pltpu.VMEM((4 * own, hidden), BF16),
            pltpu.VMEM((2, own, width), BF16),
            pltpu.VMEM((2, 2, own, width), BF16),
            pltpu.VMEM((2, 2, own, width), BF16),
            pltpu.VMEM((2, own, width), BF16),
            pltpu.VMEM((2, 4 * own, hidden), F32),
            pltpu.VMEM((groups, 4, batch, hidden), BF16),
            pltpu.VMEM((groups, 2, batch, hidden), BF16),
            pltpu.VMEM((own, width), F32),
            pltpu.VMEM((4, 8, length), F32),
            pltpu.VMEM((length, 128), F32),
            pltpu.VMEM((top_count, groups, own, batch), BF16),
            pltpu.VMEM((own, own), F32),
            pltpu.VMEM((top_count, own), jnp.int32),
            dma((7,)),
            dma((2,)),
            dma((4,)),
            dma((2,)),
            dma((4,)),
            dma((2,)),
            dma((2,)),
            dma((2,)),
            dma((CHUNKS,)),
            dma((CHUNKS,)),
            dma((2, CHUNKS)),
            dma((2, CHUNKS)),
            dma((2, 2)),
            dma((2, 2)),
            dma((groups, ep_count)),
            dma((groups, ep_count)),
            dma((groups,)),
            dma((groups,)),
            dma((groups, ep_count)),
            dma((groups, ep_count)),
            dma((groups, 2)),
            dma((groups, 2)),
            dma((groups, ep_count)),
            dma((groups, ep_count)),
        ],
        compiler_params=pltpu.CompilerParams(
            collective_id=0, has_side_effects=True, vmem_limit_bytes=67043328
        ),
    )(
        value_in,
        gate_in,
        conv_taps,
        conv_bias[None],
        ln_gain[None],
        ln_bias[None],
        norm_gain[None],
        routes.T,
        route_weights.T,
        out_proj,
        tokens_b,
        expert_gate[0],
        expert_up[0],
        expert_down[0],
        shared_gate,
        shared_up,
        shared_down,
    )


def solution(mesh):
    return jax.shard_map(
        lambda *args: tuple(per_device(*args)),
        mesh=mesh,
        in_specs=(
            P("ep", "tp"),
            P("ep", "tp"),
            P(None, "tp"),
            P("tp"),
            P("tp"),
            P("tp"),
            P("tp", None),
            P("ep", None),
            P(),
            P(("ep", "tp"), None),
            P(("ep", "tp"), None),
            P("ep", None, "tp"),
            P("ep", None, "tp"),
            P("ep", "tp", None),
            P(None, "tp"),
            P(None, "tp"),
            P("tp", None),
        ),
        out_specs=(P(("ep", "tp"), None), P(("ep", "tp"), None)),
        check_vma=False,
    )
```

```python
import jax
import jax.numpy as jnp
from jax import lax
from jax.experimental import pallas as pl
from jax.experimental.pallas import tpu as pltpu
from jax.sharding import PartitionSpec as P

MESH = pl.DeviceIdType.MESH
EPSILON = 1e-06
CHUNKS = 4
PIECES = 8
TILE = 256
STEP = 32
UNIT = 16
RIM = 32
F32, BF16 = jnp.float32, jnp.bfloat16


def dot(a, b):
    return jnp.dot(a, b, preferred_element_type=F32)


def silu(v):
    return v * jax.nn.sigmoid(v)


def aligned(i, size):
    return pl.ds(pl.multiple_of(i * size, size), size)


def kernel(
    value,
    gate,
    taps,
    bias,
    ln_gain,
    ln_bias,
    norm_gain,
    routes,
    share,
    out_proj,
    tokens,
    expert_gate,
    expert_up,
    expert_down,
    shared_gate,
    shared_up,
    shared_down,
    mixer_own,
    mixer_near,
    mixer_far,
    out_ref,
    wbuf,
    opbuf,
    dbuf,
    downs,
    tok,
    box,
    dup,
    rows,
    frows,
    ret,
    pad,
    act,
    hs,
    ns,
    kept,
    nr,
    arr,
    sacc,
    hid,
    hfar,
    total_out,
    stat,
    cols_st,
    choice,
    share_cols,
    picks,
    froutes,
    load,
    put_sem,
    tok_load,
    halo_sem,
    stat_sem,
    route_sem,
    w_send,
    w_recv,
    down_send,
    down_recv,
    near_send,
    near_recv,
    rs_near,
    rs_far,
    go_send,
    go_recv,
    dup_send,
    dup_recv,
    f_send,
    f_recv,
    h_send,
    h_recv,
    ret_send,
    ret_recv,
):
    me, t = lax.axis_index("ep"), lax.axis_index("tp")
    count = lax.axis_size("ep")
    groups = box.shape[0]
    own = share.shape[1]
    length, width = value.shape[0], tok.shape[1]
    chunk = width // CHUNKS
    batch = count * UNIT
    core, low = lax.rem(t, 2), t // 2
    near = {"tp": t + 1 - 2 * core}
    far = {"tp": lax.rem(t + 2, 4)}
    far_t = lax.rem(t + 2, 4)
    base = (me // 2) * 2
    partner = base + 1 - lax.rem(me, 2)
    hidden = hs.shape[1]
    tiles = width // TILE

    def remote(src, dst, send, recv, to):
        return pltpu.make_async_remote_copy(
            src_ref=src, dst_ref=dst, send_sem=send, recv_sem=recv, device_id=to, device_id_type=MESH
        )

    def fetch(src, dst, i):
        return pltpu.make_async_copy(src, dst, load.at[i])

    def cols(c):
        return pl.ds(c * chunk, chunk)

    barrier = pltpu.get_barrier_semaphore()
    pl.semaphore_signal(barrier, inc=1, device_id=near, device_id_type=MESH)
    pl.semaphore_signal(barrier, inc=1, device_id=far, device_id_type=MESH)

    @pl.loop(1, count)
    def _(j):
        pl.semaphore_signal(
            barrier, inc=1, device_id={"ep": lax.rem(me + j, count)}, device_id_type=MESH
        )

    def tokens_load(b):
        return pltpu.make_async_copy(tokens.at[aligned(b, own)], tok.at[aligned(b, own)], tok_load.at[b])

    tokens_load(t).start()
    tokens_load(far_t).start()
    get_sg = fetch(shared_gate, wbuf.at[0], 0)
    get_su = fetch(shared_up, wbuf.at[2], 1)
    get_sd = fetch(shared_down, opbuf.at[pl.ds(0, hidden)], 2)
    get_down = fetch(expert_down, dbuf, 6)
    get_sg.start()
    get_su.start()
    tokens_load(lax.rem(t + 1, 4)).start()
    tokens_load(lax.rem(t + 3, 4)).start()
    get_sd.start()
    get_down.start()
    pl.semaphore_wait(barrier, count + 1)

    routes_far = remote(routes, froutes, route_sem.at[0], route_sem.at[1], far)
    gate_near = remote(expert_gate, wbuf.at[1], w_send.at[0], w_recv.at[0], near)
    up_near = remote(expert_up, wbuf.at[3], w_send.at[1], w_recv.at[1], near)
    down_far = [
        remote(expert_down.at[:, cols(c)], downs.at[0, :, cols(c)], down_send.at[c], down_recv.at[c], far)
        for c in range(CHUNKS)
    ]
    down_near = [
        remote(
            expert_down.at[:, cols(c)],
            downs.at[1, :, cols(c)],
            near_send.at[0, c],
            near_recv.at[0, c],
            near,
        )
        for c in range(CHUNKS)
    ]
    down_on = [
        remote(
            downs.at[0, :, cols(c)],
            downs.at[2, :, cols(c)],
            near_send.at[1, c],
            near_recv.at[1, c],
            near,
        )
        for c in range(CHUNKS)
    ]
    routes_far.start()
    down_far[0].start()
    down_far[1].start()
    down_far[2].start()
    down_far[3].start()
    gate_near.start()
    up_near.start()
    for c in range(CHUNKS):
        down_near[c].start()

    @pl.loop(0, length // STEP)
    def _(i):
        at = aligned(i, STEP)
        gated = value[at, :].astype(F32) * jax.nn.sigmoid(gate[at, :].astype(F32))
        pad[aligned(i + 1, STEP), :] = gated.astype(BF16).astype(F32)

    def halo(to):
        return remote(
            pad.at[pl.ds(length, RIM)], pad.at[pl.ds(0, RIM)], halo_sem.at[0], halo_sem.at[1], {"ep": to}
        )

    @pl.when(me < count - 1)
    def _():
        halo(lax.rem(me + 1, count)).start()

    @pl.when(me == 0)
    def _():
        pad[pl.ds(0, RIM), :] = jnp.zeros((RIM, pad.shape[1]), F32)

    def normalize(b):
        tokens_load(b).wait()

        @pl.loop(0, own // 16)
        def _(i):
            at = pl.ds(pl.multiple_of(b * own + i * 16, 16), 16)
            x = tok[at, :].astype(F32)
            scale = lax.rsqrt(jnp.mean(x * x, axis=1, keepdims=True) + EPSILON)
            tok[at, :] = (x * scale * norm_gain[...]).astype(BF16)

    def tall(wide):
        return jnp.concatenate([wide, jnp.zeros((own - wide.shape[0], own), F32)], axis=0).T

    def placed(ids):
        lanes = lax.broadcasted_iota(jnp.int32, (own, own), 1).astype(F32)
        columns = tall(ids.astype(F32))
        chosen = [columns[:, k : k + 1] for k in range(ids.shape[0])]
        names = [(lanes == r).astype(F32) for r in chosen]
        before = lax.broadcasted_iota(jnp.int32, (own, own), 1) < lax.broadcasted_iota(
            jnp.int32, (own, own), 0
        )
        earlier = dot(before.astype(F32).astype(BF16), sum(names).astype(BF16))
        return [
            (r, jnp.sum(earlier * name, axis=1, keepdims=True)) for r, name in zip(chosen, names)
        ]

    normalize(t)
    share_cols[...] = tall(share[...])
    places = lax.broadcasted_iota(jnp.int32, (own, groups * batch), 1).astype(F32)
    anywhere = jnp.zeros((own, groups * batch), F32)
    for k, (r, place) in enumerate(placed(routes[...])):
        spot = place + UNIT * (r + (count - 1) * jnp.floor(place * (1 / UNIT)))
        chosen = (places == spot).astype(F32)
        anywhere = anywhere + chosen
        for g in range(groups):
            choice[k, g] = chosen[:, g * batch : (g + 1) * batch].astype(BF16)
    picks[...] = anywhere.T.astype(BF16)

    def going(g, to):
        return remote(box.at[g, to], rows.at[g, me], go_send.at[g, to], go_recv.at[g, me], {"ep": to})

    def came(g, source):
        return remote(
            box.at[g, source], rows.at[g, source], go_send.at[g, source], go_recv.at[g, source], {"ep": source}
        )

    def gather_rows(g):
        @pl.loop(0, tiles)
        def _(i):
            at = aligned(i, TILE)
            part = picks[g * batch : (g + 1) * batch]
            box[g, :, :, at] = dot(part, tok[aligned(t, own), at]).astype(BF16).reshape(count, UNIT, TILE)

        rows[g, me] = box[g, me]

    def send_rows(g):
        @pl.loop(1, count)
        def _(j):
            going(g, lax.rem(me + j, count)).start()

    gather_rows(0)
    send_rows(0)

    normalize(far_t)
    routes_far.wait()
    spots = lax.broadcasted_iota(jnp.int32, (own, own), 1).astype(F32)
    anywhere = jnp.zeros((own, own), F32)
    first_of_pair = base.astype(F32)
    for r, place in placed(froutes[...]):
        inside = (r - first_of_pair >= 0) & (r - first_of_pair <= 1)
        spot = place + UNIT * (r - first_of_pair + jnp.floor(place * (1 / UNIT)))
        anywhere = anywhere + jnp.where(inside & (spots == spot), 1.0, 0.0)
    pick = anywhere.T.astype(BF16)[: groups * 2 * UNIT]

    @pl.loop(0, tiles)
    def _(i):
        at = aligned(i, TILE)
        dup[:, :, :, at] = (
            dot(pick, tok[aligned(far_t, own), at]).astype(BF16).reshape(groups, 2, UNIT, TILE)
        )

    doubles = [
        remote(
            dup.at[g, partner - base], frows.at[g, me], dup_send.at[g], dup_recv.at[g], {"ep": partner}
        )
        for g in range(groups)
    ]
    for g in range(groups):
        doubles[g].start()
        frows[g, me] = dup[g, me - base]

    if groups > 1:
        gather_rows(1)

    @pl.when(me < count - 1)
    def _():
        halo(lax.rem(me + 1, count)).wait_send()

    @pl.when(me > 0)
    def _():
        halo(lax.rem(me + 1, count)).wait_recv()

    tap_count = taps.shape[0]
    first = RIM - (tap_count - 1)

    @pl.loop(0, length // STEP)
    def _(i):
        window = pad[pl.ds(pl.multiple_of(i * STEP, STEP), STEP + RIM), :]
        total = jnp.zeros((STEP, window.shape[1]), F32) + bias[...]
        for s in range(8):
            turned = pltpu.roll(window, STEP + RIM - s, 0) if s else window
            for q in range((RIM + 8) // 8):
                j = s + 8 * q - first
                if 0 <= j < tap_count:
                    total = total + taps[j : j + 1, :] * turned[8 * q : 8 * q + STEP]
        pad[aligned(i, STEP), :] = total
        lane = lax.broadcasted_iota(jnp.int32, (STEP, 128), 1)
        plain = jnp.sum(total, axis=1, keepdims=True)
        square = jnp.sum(total * total, axis=1, keepdims=True)
        cols_st[aligned(i, STEP), :] = jnp.where(
            lane == 0, plain, jnp.where(lane == 1, square, 0.0)
        )

    stat[0] = cols_st[...].T[:8]
    stat_near = remote(stat.at[0], stat.at[1], stat_sem.at[0], stat_sem.at[1], near)
    stat_near.start()

    normalize(lax.rem(t + 1, 4))
    normalize(lax.rem(t + 3, 4))
    stat_near.wait()
    stat[2] = stat[0] + stat[1]
    stat_far = remote(stat.at[2], stat.at[3], stat_sem.at[2], stat_sem.at[3], far)
    stat_far.start()
    get_sg.wait()
    get_su.wait()
    sacc[...] = jnp.zeros_like(sacc)

    @pl.loop(0, CHUNKS)
    def _(k):
        at = aligned(k, chunk)
        sacc[0] += dot(tok[:, at], wbuf[0, at, :])
        sacc[1] += dot(tok[:, at], wbuf[2, at, :])

    get_own_gate = fetch(expert_gate, wbuf.at[0], 3)
    get_own_up = fetch(expert_up, wbuf.at[2], 4)
    get_own_gate.start()
    get_own_up.start()
    hs[...] = (silu(sacc[0]) * sacc[1]).astype(BF16)

    def outside(j):
        return lax.rem(base + 2 + j, count)

    def forward(g, source):
        return remote(
            rows.at[g, source], frows.at[g, source], f_send.at[g, source], f_recv.at[g, source], far
        )

    def forward_some(g, start, stop):
        @pl.loop(start, stop)
        def _(j):
            came(g, outside(j)).wait_recv()
            forward(g, outside(j)).start()

    def forward_group(g):
        forward_some(g, 0, count - 2)
        came(g, partner).wait_recv()

    def far_ready(g):
        doubles[g].wait_recv()

        @pl.loop(0, count - 2)
        def _(j):
            forward(g, outside(j)).wait()

    def ffn(source, g, slot):
        lhs = source.at[g]
        gate_sum = jnp.zeros((batch, hidden), F32)
        up_sum = jnp.zeros((batch, hidden), F32)

        def step(k, sums):
            at = aligned(k, chunk)
            x = lhs[:, :, at].reshape(batch, chunk)
            return sums[0] + dot(x, wbuf[slot, at, :]), sums[1] + dot(x, wbuf[slot + 2, at, :])

        gate_sum, up_sum = lax.fori_loop(0, CHUNKS, step, (gate_sum, up_sum))
        return (silu(gate_sum) * up_sum).astype(BF16)

    def own_part(g):
        hid[g, 0] = ffn(rows, g, 0)
        hid[g, 2] = ffn(rows, g, 1)

    hidden_far = [
        [
            remote(hfar.at[g, n], hid.at[g, 1 + 2 * n], h_send.at[g, n], h_recv.at[g, n], far)
            for n in range(2)
        ]
        for g in range(groups)
    ]

    def far_part(g):
        far_ready(g)
        for n in range(2):
            hfar[g, n] = ffn(frows, g, n)
            hidden_far[g][n].start()

    def halves(which, lhs, depth):
        @pl.loop(0, tiles)
        def _(i):
            at = aligned(i, TILE)
            for j in range(2):
                block = aligned(2 * j + 1 - core, own)
                ns[j, :, at] = dot(lhs[block, :], opbuf[pl.ds(0, depth), at]).astype(BF16)
            for j in range(2):
                block = aligned(2 * j + core, own)
                kept[which, j, :, at] = dot(lhs[block, :], opbuf[pl.ds(0, depth), at]).astype(BF16)

    to_near = [
        remote(ns, nr.at[which], rs_near.at[which, 0], rs_near.at[which, 1], near) for which in range(2)
    ]
    piece = width // PIECES

    def crossing(which, c, into):
        return remote(
            kept.at[which, 1 - low, :, pl.ds(c * piece, piece)],
            into.at[:, pl.ds(c * piece, piece)],
            rs_far.at[which, 0, c],
            rs_far.at[which, 1, c],
            far,
        )

    shared_cross = [crossing(0, c, arr) for c in range(PIECES)]
    mixer_cross = [crossing(1, c, mixer_far) for c in range(PIECES)]

    def joined(which):
        to_near[which].wait_recv()

        @pl.loop(0, own // 16)
        def _(i):
            at = aligned(i, 16)
            kept[which, 1 - low, at, :] = (
                kept[which, 1 - low, at, :].astype(F32) + nr[which, 1 - low, at, :].astype(F32)
            ).astype(BF16)

    def back(g, to):
        return remote(box.at[g, to], ret.at[g, me], ret_send.at[g, to], ret_recv.at[g, me], {"ep": to})

    def products(g):
        @pl.loop(1, count)
        def _(j):
            came(g, lax.rem(me + j, count)).wait_send()

        for n in range(2):
            hidden_far[g][n].wait()

        @pl.loop(0, tiles)
        def _(i):
            at = aligned(i, TILE)
            total = dot(hid[g, 0], dbuf[:, at])
            for piece in range(3):
                total += dot(hid[g, piece + 1], downs[piece, :, at])
            box[g, :, :, at] = total.astype(BF16).reshape(count, UNIT, TILE)

        @pl.loop(1, count)
        def _(j):
            back(g, lax.rem(me + j, count)).start()

        ret[g, me] = box[g, me]

    def combine(g):
        @pl.loop(1, count)
        def _(j):
            source = lax.rem(me + j, count)
            remote(
                box.at[g, source],
                ret.at[g, source],
                ret_send.at[g, source],
                ret_recv.at[g, source],
                {"ep": source},
            ).wait()

        @pl.loop(0, tiles)
        def _(i):
            at = aligned(i, TILE)
            back_rows = ret[g, :, :, at].reshape(batch, TILE)
            total = jnp.zeros((own, TILE), F32)
            for k in range(choice.shape[0]):
                total += dot(choice[k, g], back_rows) * share_cols[:, k : k + 1]
            if g:
                total += total_out[:, at]
            if g == groups - 1:
                arr[:, at] = (total + ended(at).astype(F32)).astype(BF16)
            else:
                total_out[:, at] = total

    def ended(at):
        return (
            kept[0, low, :, at].astype(F32) + nr[0, low, :, at].astype(F32) + arr[:, at].astype(F32)
        ).astype(BF16)

    def normed():
        stat_far.wait()
        total = stat[2] + stat[3]
        cols_st[...] = jnp.concatenate([total, jnp.zeros((120, length), F32)], axis=0).T
        channels = pad.shape[1] * 4

        @pl.loop(0, length // STEP)
        def _(i):
            at = aligned(i, STEP)
            average = cols_st[at, 0:1] / channels
            variance = cols_st[at, 1:2] / channels - average * average
            scale = lax.rsqrt(variance + EPSILON)
            v = (pad[at, :] - average) * scale * ln_gain[...] + ln_bias[...]
            act[at, :] = silu(v).astype(BF16)

    def relay(c):
        down_far[c].wait()
        down_on[c].start()

    get_op = fetch(out_proj, opbuf, 5)

    if groups > 1:
        send_rows(1)
    for g in range(2, groups):
        gather_rows(g)
    forward_group(0)
    relay(0)
    relay(1)
    get_own_gate.wait()
    get_own_up.wait()
    gate_near.wait()
    up_near.wait()
    own_part(0)
    get_sd.wait()
    halves(0, hs, hidden)
    to_near[0].start()
    get_op.start()
    for g in range(2, groups):
        send_rows(g)
    relay(2)
    normed()
    get_op.wait()
    to_near[0].wait_send()
    halves(1, act, act.shape[1])
    to_near[1].start()
    joined(0)
    shared_cross[0].start()
    far_part(0)
    if groups > 1:
        forward_group(1)
        own_part(1)
    relay(3)
    get_down.wait()
    for c in range(CHUNKS):
        down_near[c].wait()
        down_on[c].wait()
    products(0)
    joined(1)
    keeps = [
        pltpu.make_async_copy(part.at[1, low], into, put_sem.at[1 + i])
        for i, (part, into) in enumerate(((kept, mixer_own), (nr, mixer_near)))
    ]
    for keep in keeps:
        keep.start()

    def finish_crossing():
        for copy in shared_cross[2:] + mixer_cross:
            copy.start()

    half = (count - 2) // 2
    for g in range(1, groups):
        if g + 1 < groups:
            forward_some(g + 1, 0, half)
        far_part(g)
        if g + 1 < groups:
            forward_some(g + 1, half, count - 2)
            came(g + 1, partner).wait_recv()
            own_part(g + 1)
            if g + 2 == groups:
                shared_cross[1].start()
        else:
            finish_crossing()
        products(g)
    if groups < 3:
        shared_cross[1].start()
    if groups == 1:
        finish_crossing()
    for g in range(groups - 1):
        combine(g)
    for g in range(groups):
        doubles[g].wait_send()
    to_near[1].wait_send()
    for copy in shared_cross:
        copy.wait()
    combine(groups - 1)
    put = pltpu.make_async_copy(arr, out_ref, put_sem.at[0])
    put.start()
    for keep in keeps:
        keep.wait()
    put.wait()
    for copy in mixer_cross:
        copy.wait()


def last_kernel(first, second, third, routed, mixer_ref, experts_ref):
    total = first[...].astype(F32) + second[...].astype(F32) + third[...].astype(F32)
    mixer_ref[...] = total.astype(BF16)
    experts_ref[...] = routed[...]


def per_device(
    value_in,
    gate_in,
    conv_taps,
    conv_bias,
    ln_gain,
    ln_bias,
    out_proj,
    tokens_b,
    norm_gain,
    routes,
    route_weights,
    expert_gate,
    expert_up,
    expert_down,
    shared_gate,
    shared_up,
    shared_down,
):
    ep_count = lax.axis_size("ep")
    own, top_count = routes.shape
    length, channels = value_in.shape
    width, hidden = tokens_b.shape[1], expert_down.shape[1]
    cap = 3 * own * top_count // (2 * ep_count)
    groups = -(-cap // UNIT)
    batch = ep_count * UNIT
    anywhere = pl.BlockSpec(memory_space=pl.ANY)
    vmem = pl.BlockSpec(memory_space=pltpu.VMEM)
    dma = pltpu.SemaphoreType.DMA
    mail = pltpu.VMEM((groups, ep_count, UNIT, width), BF16)
    *mixer_parts, experts_out = pl.pallas_call(
        kernel,
        out_shape=[jax.ShapeDtypeStruct((own, width), BF16)] * 4,
        in_specs=[vmem] * 9 + [anywhere] * 8,
        out_specs=[anywhere] * 4,
        scratch_shapes=[
            pltpu.VMEM((4, width, hidden), BF16),
            pltpu.VMEM((max(channels, hidden), width), BF16),
            pltpu.VMEM((hidden, width), BF16),
            pltpu.VMEM((3, hidden, width), BF16),
            pltpu.VMEM((4 * own, width), BF16),
            mail,
            pltpu.VMEM((groups, 2, UNIT, width), BF16),
            mail,
            mail,
            mail,
            pltpu.VMEM((length + RIM, channels), F32),
            pltpu.VMEM((length, channels), BF16),
            pltpu.VMEM((4 * own, hidden), BF16),
            pltpu.VMEM((2, own, width), BF16),
            pltpu.VMEM((2, 2, own, width), BF16),
            pltpu.VMEM((2, 2, own, width), BF16),
            pltpu.VMEM((own, width), BF16),
            pltpu.VMEM((2, 4 * own, hidden), F32),
            pltpu.VMEM((groups, 4, batch, hidden), BF16),
            pltpu.VMEM((groups, 2, batch, hidden), BF16),
            pltpu.VMEM((own, width), F32),
            pltpu.VMEM((4, 8, length), F32),
            pltpu.VMEM((length, 128), F32),
            pltpu.VMEM((top_count, groups, own, batch), BF16),
            pltpu.VMEM((own, own), F32),
            pltpu.VMEM((groups * batch, own), BF16),
            pltpu.VMEM((top_count, own), jnp.int32),
            dma((7,)),
            dma((3,)),
            dma((4,)),
            dma((2,)),
            dma((4,)),
            dma((2,)),
            dma((2,)),
            dma((2,)),
            dma((CHUNKS,)),
            dma((CHUNKS,)),
            dma((2, CHUNKS)),
            dma((2, CHUNKS)),
            dma((2, 2)),
            dma((2, 2, PIECES)),
            dma((groups, ep_count)),
            dma((groups, ep_count)),
            dma((groups,)),
            dma((groups,)),
            dma((groups, ep_count)),
            dma((groups, ep_count)),
            dma((groups, 2)),
            dma((groups, 2)),
            dma((groups, ep_count)),
            dma((groups, ep_count)),
        ],
        compiler_params=pltpu.CompilerParams(
            collective_id=0, has_side_effects=True, vmem_limit_bytes=67043328
        ),
    )(
        value_in,
        gate_in,
        conv_taps,
        conv_bias[None],
        ln_gain[None],
        ln_bias[None],
        norm_gain[None],
        routes.T,
        route_weights.T,
        out_proj,
        tokens_b,
        expert_gate[0],
        expert_up[0],
        expert_down[0],
        shared_gate,
        shared_up,
        shared_down,
    )
    blocks = pl.BlockSpec((own, width // CHUNKS), lambda i: (0, i))
    return pl.pallas_call(
        last_kernel,
        grid=(CHUNKS,),
        out_shape=[jax.ShapeDtypeStruct((own, width), BF16)] * 2,
        in_specs=[blocks] * 4,
        out_specs=[blocks] * 2,
    )(*mixer_parts, experts_out)


def solution(mesh):
    return jax.shard_map(
        lambda *args: tuple(per_device(*args)),
        mesh=mesh,
        in_specs=(
            P("ep", "tp"),
            P("ep", "tp"),
            P(None, "tp"),
            P("tp"),
            P("tp"),
            P("tp"),
            P("tp", None),
            P("ep", None),
            P(),
            P(("ep", "tp"), None),
            P(("ep", "tp"), None),
            P("ep", None, "tp"),
            P("ep", None, "tp"),
            P("ep", "tp", None),
            P(None, "tp"),
            P(None, "tp"),
            P("tp", None),
        ),
        out_specs=(P(("ep", "tp"), None), P(("ep", "tp"), None)),
        check_vma=False,
    )
```

```python
import jax
import jax.numpy as jnp
from jax import lax
from jax.experimental import pallas as pl
from jax.experimental.pallas import tpu as pltpu
from jax.sharding import PartitionSpec as P

MESH = pl.DeviceIdType.MESH
EPSILON = 1e-06
CHUNKS = 4
PIECES = 8
EARLY = 2
TILE = 256
STEP = 32
UNIT = 16
HALF = 4
RIM = 32
F32, BF16 = jnp.float32, jnp.bfloat16


def dot(a, b):
    return jnp.dot(a, b, preferred_element_type=F32)


def silu(v):
    return v * jax.nn.sigmoid(v)


def aligned(i, size):
    return pl.ds(pl.multiple_of(i * size, size), size)


def kernel(
    value,
    gate,
    taps,
    bias,
    ln_gain,
    ln_bias,
    norm_gain,
    routes,
    share,
    out_proj,
    tokens,
    expert_gate,
    expert_up,
    expert_down,
    shared_gate,
    shared_up,
    shared_down,
    mixer_ref,
    out_ref,
    wbuf,
    opbuf,
    dbuf,
    downs,
    tok,
    box,
    dup,
    rows,
    frows,
    ret,
    pad,
    act,
    hs,
    ns,
    kept,
    nr,
    arr,
    mix,
    sacc,
    hid,
    hfar,
    total_out,
    stat,
    cols_st,
    choice,
    share_cols,
    picks,
    froutes,
    load,
    put_sem,
    tok_load,
    halo_sem,
    stat_sem,
    route_sem,
    w_send,
    w_recv,
    down_send,
    down_recv,
    near_send,
    near_recv,
    rs_near,
    rs_far,
    go_send,
    go_recv,
    dup_send,
    dup_recv,
    f_send,
    f_recv,
    h_send,
    h_recv,
    ret_send,
    ret_recv,
):
    me, t = lax.axis_index("ep"), lax.axis_index("tp")
    count = lax.axis_size("ep")
    groups = box.shape[0]
    own = share.shape[1]
    length, width = value.shape[0], tok.shape[1]
    chunk = width // CHUNKS
    batch = count * UNIT
    core, low = lax.rem(t, 2), t // 2
    near = {"tp": t + 1 - 2 * core}
    far = {"tp": lax.rem(t + 2, 4)}
    far_t = lax.rem(t + 2, 4)
    base = (me // HALF) * HALF
    place_in = me - base
    hidden = hs.shape[1]
    tiles = width // TILE

    def remote(src, dst, send, recv, to):
        return pltpu.make_async_remote_copy(
            src_ref=src, dst_ref=dst, send_sem=send, recv_sem=recv, device_id=to, device_id_type=MESH
        )

    def fetch(src, dst, i):
        return pltpu.make_async_copy(src, dst, load.at[i])

    def cols(c):
        return pl.ds(c * chunk, chunk)

    barrier = pltpu.get_barrier_semaphore()
    pl.semaphore_signal(barrier, inc=1, device_id=near, device_id_type=MESH)
    pl.semaphore_signal(barrier, inc=1, device_id=far, device_id_type=MESH)

    @pl.loop(1, count)
    def _(j):
        pl.semaphore_signal(
            barrier, inc=1, device_id={"ep": lax.rem(me + j, count)}, device_id_type=MESH
        )

    def tokens_load(b):
        return pltpu.make_async_copy(tokens.at[aligned(b, own)], tok.at[aligned(b, own)], tok_load.at[b])

    tokens_load(t).start()
    tokens_load(far_t).start()
    get_sg = fetch(shared_gate, wbuf.at[0], 0)
    get_su = fetch(shared_up, wbuf.at[2], 1)
    get_sd = fetch(shared_down, opbuf.at[pl.ds(0, hidden)], 2)
    get_down = fetch(expert_down, dbuf, 6)
    get_sg.start()
    get_su.start()
    tokens_load(lax.rem(t + 1, 4)).start()
    tokens_load(lax.rem(t + 3, 4)).start()
    get_sd.start()
    get_down.start()
    pl.semaphore_wait(barrier, count + 1)

    routes_far = remote(routes, froutes, route_sem.at[0], route_sem.at[1], far)
    gate_near = remote(expert_gate, wbuf.at[1], w_send.at[0], w_recv.at[0], near)
    up_near = remote(expert_up, wbuf.at[3], w_send.at[1], w_recv.at[1], near)
    down_far = [
        remote(expert_down.at[:, cols(c)], downs.at[0, :, cols(c)], down_send.at[c], down_recv.at[c], far)
        for c in range(CHUNKS)
    ]
    down_near = [
        remote(
            expert_down.at[:, cols(c)],
            downs.at[1, :, cols(c)],
            near_send.at[0, c],
            near_recv.at[0, c],
            near,
        )
        for c in range(CHUNKS)
    ]
    down_on = [
        remote(
            downs.at[0, :, cols(c)],
            downs.at[2, :, cols(c)],
            near_send.at[1, c],
            near_recv.at[1, c],
            near,
        )
        for c in range(CHUNKS)
    ]
    routes_far.start()
    down_far[0].start()
    down_far[1].start()
    down_far[2].start()
    gate_near.start()
    up_near.start()
    for c in range(CHUNKS):
        down_near[c].start()

    @pl.loop(0, length // STEP)
    def _(i):
        at = aligned(i, STEP)
        gated = value[at, :].astype(F32) * jax.nn.sigmoid(gate[at, :].astype(F32))
        pad[aligned(i + 1, STEP), :] = gated.astype(BF16).astype(F32)

    def halo(to):
        return remote(
            pad.at[pl.ds(length, RIM)], pad.at[pl.ds(0, RIM)], halo_sem.at[0], halo_sem.at[1], {"ep": to}
        )

    @pl.when(me < count - 1)
    def _():
        halo(lax.rem(me + 1, count)).start()

    @pl.when(me == 0)
    def _():
        pad[pl.ds(0, RIM), :] = jnp.zeros((RIM, pad.shape[1]), F32)

    def normalize(b):
        tokens_load(b).wait()

        @pl.loop(0, own // 16)
        def _(i):
            at = pl.ds(pl.multiple_of(b * own + i * 16, 16), 16)
            x = tok[at, :].astype(F32)
            scale = lax.rsqrt(jnp.mean(x * x, axis=1, keepdims=True) + EPSILON)
            tok[at, :] = (x * scale * norm_gain[...]).astype(BF16)

    def tall(wide):
        return jnp.concatenate([wide, jnp.zeros((own - wide.shape[0], own), F32)], axis=0).T

    def placed(ids):
        lanes = lax.broadcasted_iota(jnp.int32, (own, own), 1).astype(F32)
        columns = tall(ids.astype(F32))
        chosen = [columns[:, k : k + 1] for k in range(ids.shape[0])]
        names = [(lanes == r).astype(F32) for r in chosen]
        before = lax.broadcasted_iota(jnp.int32, (own, own), 1) < lax.broadcasted_iota(
            jnp.int32, (own, own), 0
        )
        earlier = dot(before.astype(F32).astype(BF16), sum(names).astype(BF16))
        return [
            (r, jnp.sum(earlier * name, axis=1, keepdims=True)) for r, name in zip(chosen, names)
        ]

    normalize(t)
    share_cols[...] = tall(share[...])
    places = lax.broadcasted_iota(jnp.int32, (own, groups * batch), 1).astype(F32)
    anywhere = jnp.zeros((own, groups * batch), F32)
    for k, (r, place) in enumerate(placed(routes[...])):
        spot = place + UNIT * (r + (count - 1) * jnp.floor(place * (1 / UNIT)))
        chosen = (places == spot).astype(F32)
        anywhere = anywhere + chosen
        for g in range(groups):
            choice[k, g] = chosen[:, g * batch : (g + 1) * batch].astype(BF16)
    picks[...] = anywhere.T.astype(BF16)

    def going(g, to):
        return remote(box.at[g, to], rows.at[g, me], go_send.at[g, to], go_recv.at[g, me], {"ep": to})

    def came(g, source):
        return remote(
            box.at[g, source], rows.at[g, source], go_send.at[g, source], go_recv.at[g, source], {"ep": source}
        )

    def gather_rows(g):
        @pl.loop(0, tiles)
        def _(i):
            at = aligned(i, TILE)
            part = picks[g * batch : (g + 1) * batch]
            box[g, :, :, at] = dot(part, tok[aligned(t, own), at]).astype(BF16).reshape(count, UNIT, TILE)

        rows[g, me] = box[g, me]

    def send_rows(g):
        @pl.loop(1, count)
        def _(j):
            going(g, lax.rem(me + j, count)).start()

    gather_rows(0)
    send_rows(0)

    normalize(far_t)
    routes_far.wait()
    spot_count = -(-groups * HALF * UNIT // 128) * 128
    spots = lax.broadcasted_iota(jnp.int32, (own, spot_count), 1).astype(F32)
    anywhere = jnp.zeros((own, spot_count), F32)
    first_of_pair = base.astype(F32)
    for r, place in placed(froutes[...]):
        inside = (r - first_of_pair >= 0) & (r - first_of_pair < HALF)
        spot = place + UNIT * (r - first_of_pair + (HALF - 1) * jnp.floor(place * (1 / UNIT)))
        anywhere = anywhere + jnp.where(inside & (spots == spot), 1.0, 0.0)
    pick = anywhere.T.astype(BF16)[: groups * HALF * UNIT]

    @pl.loop(0, tiles)
    def _(i):
        at = aligned(i, TILE)
        dup[:, :, :, at] = (
            dot(pick, tok[aligned(far_t, own), at]).astype(BF16).reshape(groups, HALF, UNIT, TILE)
        )

    def double(g, j):
        to = lax.rem(place_in + j, HALF)
        return remote(
            dup.at[g, to], frows.at[g, me], dup_send.at[g, to], dup_recv.at[g, place_in], {"ep": base + to}
        )

    def doubled(g, j):
        source = lax.rem(place_in + j, HALF)
        return remote(
            dup.at[g, source],
            frows.at[g, base + source],
            dup_send.at[g, source],
            dup_recv.at[g, source],
            {"ep": base + source},
        )

    def send_doubles(g):
        @pl.loop(1, HALF)
        def _(j):
            double(g, j).start()

    for g in range(groups):
        frows[g, me] = dup[g, place_in]
    send_doubles(0)

    if groups > 1:
        gather_rows(1)

    @pl.when(me < count - 1)
    def _():
        halo(lax.rem(me + 1, count)).wait_send()

    @pl.when(me > 0)
    def _():
        halo(lax.rem(me + 1, count)).wait_recv()

    tap_count = taps.shape[0]
    first = RIM - (tap_count - 1)

    @pl.loop(0, length // STEP)
    def _(i):
        window = pad[pl.ds(pl.multiple_of(i * STEP, STEP), STEP + RIM), :]
        total = jnp.zeros((STEP, window.shape[1]), F32) + bias[...]
        for s in range(8):
            turned = pltpu.roll(window, STEP + RIM - s, 0) if s else window
            for q in range((RIM + 8) // 8):
                j = s + 8 * q - first
                if 0 <= j < tap_count:
                    total = total + taps[j : j + 1, :] * turned[8 * q : 8 * q + STEP]
        pad[aligned(i, STEP), :] = total
        lane = lax.broadcasted_iota(jnp.int32, (STEP, 128), 1)
        plain = jnp.sum(total, axis=1, keepdims=True)
        square = jnp.sum(total * total, axis=1, keepdims=True)
        cols_st[aligned(i, STEP), :] = jnp.where(
            lane == 0, plain, jnp.where(lane == 1, square, 0.0)
        )

    stat[0] = cols_st[...].T[:8]
    stat_near = remote(stat.at[0], stat.at[1], stat_sem.at[0], stat_sem.at[1], near)
    stat_near.start()

    normalize(lax.rem(t + 1, 4))
    normalize(lax.rem(t + 3, 4))
    stat_near.wait()
    stat[2] = stat[0] + stat[1]
    stat_far = remote(stat.at[2], stat.at[3], stat_sem.at[2], stat_sem.at[3], far)
    stat_far.start()
    down_far[3].start()
    get_sg.wait()
    get_su.wait()
    sacc[...] = jnp.zeros_like(sacc)

    @pl.loop(0, CHUNKS)
    def _(k):
        at = aligned(k, chunk)
        sacc[0] += dot(tok[:, at], wbuf[0, at, :])
        sacc[1] += dot(tok[:, at], wbuf[2, at, :])

    get_own_gate = fetch(expert_gate, wbuf.at[0], 3)
    get_own_up = fetch(expert_up, wbuf.at[2], 4)
    get_own_gate.start()
    get_own_up.start()
    hs[...] = (silu(sacc[0]) * sacc[1]).astype(BF16)

    def outside(j):
        return lax.rem(base + HALF + j, count)

    def forward(g, source):
        return remote(
            rows.at[g, source], frows.at[g, source], f_send.at[g, source], f_recv.at[g, source], far
        )

    def forward_some(g, start, stop):
        @pl.loop(start, stop)
        def _(j):
            came(g, outside(j)).wait_recv()
            forward(g, outside(j)).start()

    def near_came(g):
        @pl.loop(1, HALF)
        def _(j):
            came(g, base + lax.rem(place_in + j, HALF)).wait_recv()

    def forward_group(g):
        forward_some(g, 0, count - HALF)
        near_came(g)

    def far_ready(g):
        @pl.loop(1, HALF)
        def _(j):
            doubled(g, j).wait()

        @pl.loop(0, count - HALF)
        def _(j):
            forward(g, outside(j)).wait()

    def ffn(source, g, slot):
        lhs = source.at[g]
        gate_sum = jnp.zeros((batch, hidden), F32)
        up_sum = jnp.zeros((batch, hidden), F32)

        def step(k, sums):
            at = aligned(k, chunk)
            x = lhs[:, :, at].reshape(batch, chunk)
            return sums[0] + dot(x, wbuf[slot, at, :]), sums[1] + dot(x, wbuf[slot + 2, at, :])

        gate_sum, up_sum = lax.fori_loop(0, CHUNKS, step, (gate_sum, up_sum))
        return (silu(gate_sum) * up_sum).astype(BF16)

    def own_part(g):
        hid[g, 0] = ffn(rows, g, 0)
        hid[g, 2] = ffn(rows, g, 1)

    hidden_far = [
        [
            remote(hfar.at[g, n], hid.at[g, 1 + 2 * n], h_send.at[g, n], h_recv.at[g, n], far)
            for n in range(2)
        ]
        for g in range(groups)
    ]

    def far_part(g):
        far_ready(g)
        for n in range(2):
            hfar[g, n] = ffn(frows, g, n)
            hidden_far[g][n].start()

    def halves(which, lhs, depth):
        @pl.loop(0, tiles)
        def _(i):
            at = aligned(i, TILE)
            for j in range(2):
                block = aligned(2 * j + 1 - core, own)
                ns[j, :, at] = dot(lhs[block, :], opbuf[pl.ds(0, depth), at]).astype(BF16)
            for j in range(2):
                block = aligned(2 * j + core, own)
                kept[which, j, :, at] = dot(lhs[block, :], opbuf[pl.ds(0, depth), at]).astype(BF16)

    to_near = [
        remote(ns, nr.at[which], rs_near.at[which, 0], rs_near.at[which, 1], near) for which in range(2)
    ]
    piece = width // PIECES

    def crossing(which, c, into):
        return remote(
            kept.at[which, 1 - low, :, pl.ds(c * piece, piece)],
            into.at[:, pl.ds(c * piece, piece)],
            rs_far.at[which, 0, c],
            rs_far.at[which, 1, c],
            far,
        )

    shared_cross = [crossing(0, c, arr) for c in range(PIECES)]
    mixer_cross = [crossing(1, c, mix) for c in range(PIECES)]

    def joined(which):
        to_near[which].wait_recv()

        @pl.loop(0, own // 16)
        def _(i):
            at = aligned(i, 16)
            kept[which, 1 - low, at, :] = (
                kept[which, 1 - low, at, :].astype(F32) + nr[which, 1 - low, at, :].astype(F32)
            ).astype(BF16)

    def back(g, to):
        return remote(box.at[g, to], ret.at[g, me], ret_send.at[g, to], ret_recv.at[g, me], {"ep": to})

    def products(g):
        @pl.loop(1, count)
        def _(j):
            came(g, lax.rem(me + j, count)).wait_send()

        for n in range(2):
            hidden_far[g][n].wait()

        @pl.loop(0, tiles)
        def _(i):
            at = aligned(i, TILE)
            total = dot(hid[g, 0], dbuf[:, at])
            for piece in range(3):
                total += dot(hid[g, piece + 1], downs[piece, :, at])
            box[g, :, :, at] = total.astype(BF16).reshape(count, UNIT, TILE)

        @pl.loop(1, count)
        def _(j):
            back(g, lax.rem(me + j, count)).start()

        ret[g, me] = box[g, me]

    def combine(g):
        @pl.loop(1, count)
        def _(j):
            source = lax.rem(me + j, count)
            remote(
                box.at[g, source],
                ret.at[g, source],
                ret_send.at[g, source],
                ret_recv.at[g, source],
                {"ep": source},
            ).wait()

        @pl.loop(0, tiles)
        def _(i):
            at = aligned(i, TILE)
            back_rows = ret[g, :, :, at].reshape(batch, TILE)
            total = jnp.zeros((own, TILE), F32)
            for k in range(choice.shape[0]):
                total += dot(choice[k, g], back_rows) * share_cols[:, k : k + 1]
            if g:
                total += total_out[:, at]
            if g == groups - 1:
                arr[:, at] = (total + ended(at).astype(F32)).astype(BF16)
            else:
                total_out[:, at] = total

    def ended(at, which=0, came_from=arr):
        return (
            kept[which, low, :, at].astype(F32)
            + nr[which, low, :, at].astype(F32)
            + came_from[:, at].astype(F32)
        ).astype(BF16)

    def normed():
        stat_far.wait()
        total = stat[2] + stat[3]
        cols_st[...] = jnp.concatenate([total, jnp.zeros((120, length), F32)], axis=0).T
        channels = pad.shape[1] * 4

        @pl.loop(0, length // STEP)
        def _(i):
            at = aligned(i, STEP)
            average = cols_st[at, 0:1] / channels
            variance = cols_st[at, 1:2] / channels - average * average
            scale = lax.rsqrt(variance + EPSILON)
            v = (pad[at, :] - average) * scale * ln_gain[...] + ln_bias[...]
            act[at, :] = silu(v).astype(BF16)

    def relay(c):
        down_far[c].wait()
        down_on[c].start()

    get_op = fetch(out_proj, opbuf, 5)

    if groups > 1:
        send_rows(1)
        send_doubles(1)
    for g in range(2, groups):
        gather_rows(g)
    forward_group(0)
    relay(0)
    relay(1)
    get_own_gate.wait()
    get_own_up.wait()
    gate_near.wait()
    up_near.wait()
    own_part(0)
    for g in range(2, groups):
        send_rows(g)
        send_doubles(g)
    get_sd.wait()
    halves(0, hs, hidden)
    to_near[0].start()
    get_op.start()
    relay(2)
    normed()
    get_op.wait()
    to_near[0].wait_send()
    halves(1, act, act.shape[1])
    to_near[1].start()
    joined(0)
    shared_cross[0].start()
    far_part(0)
    if groups > 1:
        forward_group(1)
        own_part(1)
    relay(3)
    get_down.wait()
    for c in range(CHUNKS):
        down_near[c].wait()
        down_on[c].wait()
    products(0)
    joined(1)
    def finish_crossing():
        for copy in shared_cross[EARLY + 1 :] + mixer_cross:
            copy.start()

    for g in range(1, groups):
        if g + 2 == groups:
            shared_cross[1].start()
        far_part(g)
        if g + 1 < groups:
            forward_group(g + 1)
            if g + 2 == groups:
                shared_cross[EARLY].start()
            own_part(g + 1)
        else:
            finish_crossing()
        products(g)
    if groups < 3:
        for copy in shared_cross[1 : EARLY + 1]:
            copy.start()
    if groups == 1:
        finish_crossing()
    for g in range(groups - 1):
        combine(g)
    to_near[1].wait_send()
    for copy in shared_cross + mixer_cross:
        copy.wait()

    @pl.loop(0, tiles)
    def _(i):
        at = aligned(i, TILE)
        mix[:, at] = ended(at, 1, mix)

    put_mixer = pltpu.make_async_copy(mix, mixer_ref, put_sem.at[1])
    put_mixer.start()
    combine(groups - 1)
    put = pltpu.make_async_copy(arr, out_ref, put_sem.at[0])
    put.start()
    put_mixer.wait()
    put.wait()


def per_device(
    value_in,
    gate_in,
    conv_taps,
    conv_bias,
    ln_gain,
    ln_bias,
    out_proj,
    tokens_b,
    norm_gain,
    routes,
    route_weights,
    expert_gate,
    expert_up,
    expert_down,
    shared_gate,
    shared_up,
    shared_down,
):
    ep_count = lax.axis_size("ep")
    own, top_count = routes.shape
    length, channels = value_in.shape
    width, hidden = tokens_b.shape[1], expert_down.shape[1]
    cap = 3 * own * top_count // (2 * ep_count)
    groups = -(-cap // UNIT)
    batch = ep_count * UNIT
    anywhere = pl.BlockSpec(memory_space=pl.ANY)
    vmem = pl.BlockSpec(memory_space=pltpu.VMEM)
    dma = pltpu.SemaphoreType.DMA
    mail = pltpu.VMEM((groups, ep_count, UNIT, width), BF16)
    return pl.pallas_call(
        kernel,
        out_shape=[jax.ShapeDtypeStruct((own, width), BF16)] * 2,
        in_specs=[vmem] * 9 + [anywhere] * 8,
        out_specs=[anywhere] * 2,
        scratch_shapes=[
            pltpu.VMEM((4, width, hidden), BF16),
            pltpu.VMEM((max(channels, hidden), width), BF16),
            pltpu.VMEM((hidden, width), BF16),
            pltpu.VMEM((3, hidden, width), BF16),
            pltpu.VMEM((4 * own, width), BF16),
            mail,
            pltpu.VMEM((groups, HALF, UNIT, width), BF16),
            mail,
            mail,
            mail,
            pltpu.VMEM((length + RIM, channels), F32),
            pltpu.VMEM((length, channels), BF16),
            pltpu.VMEM((4 * own, hidden), BF16),
            pltpu.VMEM((2, own, width), BF16),
            pltpu.VMEM((2, 2, own, width), BF16),
            pltpu.VMEM((2, 2, own, width), BF16),
            pltpu.VMEM((own, width), BF16),
            pltpu.VMEM((own, width), BF16),
            pltpu.VMEM((2, 4 * own, hidden), F32),
            pltpu.VMEM((groups, 4, batch, hidden), BF16),
            pltpu.VMEM((groups, 2, batch, hidden), BF16),
            pltpu.VMEM((own, width), F32),
            pltpu.VMEM((4, 8, length), F32),
            pltpu.VMEM((length, 128), F32),
            pltpu.VMEM((top_count, groups, own, batch), BF16),
            pltpu.VMEM((own, own), F32),
            pltpu.VMEM((groups * batch, own), BF16),
            pltpu.VMEM((top_count, own), jnp.int32),
            dma((7,)),
            dma((2,)),
            dma((4,)),
            dma((2,)),
            dma((4,)),
            dma((2,)),
            dma((2,)),
            dma((2,)),
            dma((CHUNKS,)),
            dma((CHUNKS,)),
            dma((2, CHUNKS)),
            dma((2, CHUNKS)),
            dma((2, 2)),
            dma((2, 2, PIECES)),
            dma((groups, ep_count)),
            dma((groups, ep_count)),
            dma((groups, HALF)),
            dma((groups, HALF)),
            dma((groups, ep_count)),
            dma((groups, ep_count)),
            dma((groups, 2)),
            dma((groups, 2)),
            dma((groups, ep_count)),
            dma((groups, ep_count)),
        ],
        compiler_params=pltpu.CompilerParams(
            collective_id=0, has_side_effects=True, vmem_limit_bytes=67043328
        ),
    )(
        value_in,
        gate_in,
        conv_taps,
        conv_bias[None],
        ln_gain[None],
        ln_bias[None],
        norm_gain[None],
        routes.T,
        route_weights.T,
        out_proj,
        tokens_b,
        expert_gate[0],
        expert_up[0],
        expert_down[0],
        shared_gate,
        shared_up,
        shared_down,
    )


def solution(mesh):
    return jax.shard_map(
        lambda *args: tuple(per_device(*args)),
        mesh=mesh,
        in_specs=(
            P("ep", "tp"),
            P("ep", "tp"),
            P(None, "tp"),
            P("tp"),
            P("tp"),
            P("tp"),
            P("tp", None),
            P("ep", None),
            P(),
            P(("ep", "tp"), None),
            P(("ep", "tp"), None),
            P("ep", None, "tp"),
            P("ep", None, "tp"),
            P("ep", "tp", None),
            P(None, "tp"),
            P(None, "tp"),
            P("tp", None),
        ),
        out_specs=(P(("ep", "tp"), None), P(("ep", "tp"), None)),
        check_vma=False,
    )
```

```python
import jax
import jax.numpy as jnp
from jax import lax
from jax.experimental import pallas as pl
from jax.experimental.pallas import tpu as pltpu
from jax.sharding import PartitionSpec as P

MESH = pl.DeviceIdType.MESH
EPSILON = 1e-06
CHUNKS = 4
PIECES = 8
EARLY = 3
TILE = 256
STEP = 32
UNIT = 16
HALF = 4
RIM = 32
F32, BF16 = jnp.float32, jnp.bfloat16


def dot(a, b):
    return jnp.dot(a, b, preferred_element_type=F32)


def silu(v):
    return v * jax.nn.sigmoid(v)


def aligned(i, size):
    return pl.ds(pl.multiple_of(i * size, size), size)


def kernel(
    value_in,
    gate_in,
    taps,
    bias,
    ln_gain,
    ln_bias,
    norm_gain,
    routes,
    share,
    out_proj,
    tokens,
    expert_gate,
    expert_up,
    expert_down,
    shared_gate,
    shared_up,
    shared_down,
    mixer_ref,
    out_ref,
    value,
    gate,
    wbuf,
    opbuf,
    dbuf,
    downs,
    tok,
    box,
    dup,
    rows,
    frows,
    ret,
    pad,
    act,
    hs,
    ns,
    kept,
    nr,
    arr,
    mix,
    sacc,
    hid,
    hfar,
    total_out,
    stat,
    cols_st,
    choice,
    share_cols,
    picks,
    froutes,
    load,
    put_sem,
    tok_load,
    halo_sem,
    stat_sem,
    route_sem,
    w_send,
    w_recv,
    down_send,
    down_recv,
    near_send,
    near_recv,
    rs_near,
    rs_far,
    go_send,
    go_recv,
    dup_send,
    dup_recv,
    f_send,
    f_recv,
    h_send,
    h_recv,
    ret_send,
    ret_recv,
):
    me, t = lax.axis_index("ep"), lax.axis_index("tp")
    count = lax.axis_size("ep")
    groups = box.shape[0]
    own = share.shape[1]
    length, width = value.shape[0], tok.shape[1]
    chunk = width // CHUNKS
    batch = count * UNIT
    core, low = lax.rem(t, 2), t // 2
    near = {"tp": t + 1 - 2 * core}
    far = {"tp": lax.rem(t + 2, 4)}
    far_t = lax.rem(t + 2, 4)
    base = (me // HALF) * HALF
    place_in = me - base
    hidden = hs.shape[1]
    tiles = width // TILE

    def remote(src, dst, send, recv, to):
        return pltpu.make_async_remote_copy(
            src_ref=src, dst_ref=dst, send_sem=send, recv_sem=recv, device_id=to, device_id_type=MESH
        )

    def fetch(src, dst, i):
        return pltpu.make_async_copy(src, dst, load.at[i])

    def cols(c):
        return pl.ds(c * chunk, chunk)

    barrier = pltpu.get_barrier_semaphore()
    pl.semaphore_signal(barrier, inc=1, device_id=near, device_id_type=MESH)
    pl.semaphore_signal(barrier, inc=1, device_id=far, device_id_type=MESH)

    @pl.loop(1, count)
    def _(j):
        pl.semaphore_signal(
            barrier, inc=1, device_id={"ep": lax.rem(me + j, count)}, device_id_type=MESH
        )

    def tokens_load(b):
        return pltpu.make_async_copy(tokens.at[aligned(b, own)], tok.at[aligned(b, own)], tok_load.at[b])

    get_value = fetch(value_in, value, 7)
    get_gate = fetch(gate_in, gate, 8)
    get_value.start()
    get_gate.start()
    tokens_load(t).start()
    tokens_load(far_t).start()
    get_sg = fetch(shared_gate, wbuf.at[0], 0)
    get_su = fetch(shared_up, wbuf.at[2], 1)
    get_sd = fetch(shared_down, opbuf.at[pl.ds(0, hidden)], 2)
    get_down = fetch(expert_down, dbuf, 6)
    get_sg.start()
    get_su.start()
    tokens_load(lax.rem(t + 1, 4)).start()
    tokens_load(lax.rem(t + 3, 4)).start()
    get_sd.start()
    get_down.start()
    pl.semaphore_wait(barrier, count + 1)

    routes_far = remote(routes, froutes, route_sem.at[0], route_sem.at[1], far)
    gate_near = remote(expert_gate, wbuf.at[1], w_send.at[0], w_recv.at[0], near)
    up_near = remote(expert_up, wbuf.at[3], w_send.at[1], w_recv.at[1], near)
    down_far = [
        remote(expert_down.at[:, cols(c)], downs.at[0, :, cols(c)], down_send.at[c], down_recv.at[c], far)
        for c in range(CHUNKS)
    ]
    down_near = [
        remote(
            expert_down.at[:, cols(c)],
            downs.at[1, :, cols(c)],
            near_send.at[0, c],
            near_recv.at[0, c],
            near,
        )
        for c in range(CHUNKS)
    ]
    down_on = [
        remote(
            downs.at[0, :, cols(c)],
            downs.at[2, :, cols(c)],
            near_send.at[1, c],
            near_recv.at[1, c],
            near,
        )
        for c in range(CHUNKS)
    ]
    routes_far.start()
    down_far[0].start()
    down_far[1].start()
    down_far[2].start()
    gate_near.start()
    up_near.start()
    for c in range(CHUNKS):
        down_near[c].start()

    get_value.wait()
    get_gate.wait()

    @pl.loop(0, length // STEP)
    def _(i):
        at = aligned(i, STEP)
        gated = value[at, :].astype(F32) * jax.nn.sigmoid(gate[at, :].astype(F32))
        pad[aligned(i + 1, STEP), :] = gated.astype(BF16).astype(F32)

    def halo(to):
        return remote(
            pad.at[pl.ds(length, RIM)], pad.at[pl.ds(0, RIM)], halo_sem.at[0], halo_sem.at[1], {"ep": to}
        )

    @pl.when(me < count - 1)
    def _():
        halo(lax.rem(me + 1, count)).start()

    @pl.when(me == 0)
    def _():
        pad[pl.ds(0, RIM), :] = jnp.zeros((RIM, pad.shape[1]), F32)

    def normalize(b):
        tokens_load(b).wait()

        @pl.loop(0, own // 16)
        def _(i):
            at = pl.ds(pl.multiple_of(b * own + i * 16, 16), 16)
            x = tok[at, :].astype(F32)
            scale = lax.rsqrt(jnp.mean(x * x, axis=1, keepdims=True) + EPSILON)
            tok[at, :] = (x * scale * norm_gain[...]).astype(BF16)

    def tall(wide):
        return jnp.concatenate([wide, jnp.zeros((own - wide.shape[0], own), F32)], axis=0).T

    def placed(ids):
        lanes = lax.broadcasted_iota(jnp.int32, (own, own), 1).astype(F32)
        columns = tall(ids.astype(F32))
        chosen = [columns[:, k : k + 1] for k in range(ids.shape[0])]
        names = [(lanes == r).astype(F32) for r in chosen]
        before = lax.broadcasted_iota(jnp.int32, (own, own), 1) < lax.broadcasted_iota(
            jnp.int32, (own, own), 0
        )
        earlier = dot(before.astype(F32).astype(BF16), sum(names).astype(BF16))
        return [
            (r, jnp.sum(earlier * name, axis=1, keepdims=True)) for r, name in zip(chosen, names)
        ]

    normalize(t)
    share_cols[...] = tall(share[...])
    places = lax.broadcasted_iota(jnp.int32, (own, groups * batch), 1).astype(F32)
    anywhere = jnp.zeros((own, groups * batch), F32)
    for k, (r, place) in enumerate(placed(routes[...])):
        spot = place + UNIT * (r + (count - 1) * jnp.floor(place * (1 / UNIT)))
        chosen = (places == spot).astype(F32)
        anywhere = anywhere + chosen
        for g in range(groups):
            choice[k, g] = chosen[:, g * batch : (g + 1) * batch].astype(BF16)
    picks[...] = anywhere.T.astype(BF16)

    def going(g, to):
        return remote(box.at[g, to], rows.at[g, me], go_send.at[g], go_recv.at[g, me], {"ep": to})

    def came(g, source):
        return remote(
            box.at[g, source], rows.at[g, source], go_send.at[g], go_recv.at[g, source], {"ep": source}
        )

    def gather_rows(g):
        @pl.loop(0, tiles)
        def _(i):
            at = aligned(i, TILE)
            part = picks[g * batch : (g + 1) * batch]
            box[g, :, :, at] = dot(part, tok[aligned(t, own), at]).astype(BF16).reshape(count, UNIT, TILE)

        rows[g, me] = box[g, me]

    def send_rows(g):
        @pl.loop(1, count)
        def _(j):
            going(g, lax.rem(me + j, count)).start()

    gather_rows(0)
    send_rows(0)

    normalize(far_t)
    routes_far.wait()
    spot_count = -(-groups * HALF * UNIT // 128) * 128
    spots = lax.broadcasted_iota(jnp.int32, (own, spot_count), 1).astype(F32)
    anywhere = jnp.zeros((own, spot_count), F32)
    first_of_pair = base.astype(F32)
    for r, place in placed(froutes[...]):
        inside = (r - first_of_pair >= 0) & (r - first_of_pair < HALF)
        spot = place + UNIT * (r - first_of_pair + (HALF - 1) * jnp.floor(place * (1 / UNIT)))
        anywhere = anywhere + jnp.where(inside & (spots == spot), 1.0, 0.0)
    pick = anywhere.T.astype(BF16)[: groups * HALF * UNIT]

    @pl.loop(0, tiles)
    def _(i):
        at = aligned(i, TILE)
        dup[:, :, :, at] = (
            dot(pick, tok[aligned(far_t, own), at]).astype(BF16).reshape(groups, HALF, UNIT, TILE)
        )

    def double(g, j):
        to = lax.rem(place_in + j, HALF)
        return remote(
            dup.at[g, to], frows.at[g, me], dup_send.at[g, to], dup_recv.at[g, place_in], {"ep": base + to}
        )

    def doubled(g, j):
        source = lax.rem(place_in + j, HALF)
        return remote(
            dup.at[g, source],
            frows.at[g, base + source],
            dup_send.at[g, source],
            dup_recv.at[g, source],
            {"ep": base + source},
        )

    def send_doubles(g):
        @pl.loop(1, HALF)
        def _(j):
            double(g, j).start()

    for g in range(groups):
        frows[g, me] = dup[g, place_in]
    send_doubles(0)

    if groups > 1:
        gather_rows(1)

    @pl.when(me < count - 1)
    def _():
        halo(lax.rem(me + 1, count)).wait_send()

    @pl.when(me > 0)
    def _():
        halo(lax.rem(me + 1, count)).wait_recv()

    tap_count = taps.shape[0]
    first = RIM - (tap_count - 1)

    @pl.loop(0, length // STEP)
    def _(i):
        window = pad[pl.ds(pl.multiple_of(i * STEP, STEP), STEP + RIM), :]
        total = jnp.zeros((STEP, window.shape[1]), F32) + bias[...]
        for s in range(8):
            turned = pltpu.roll(window, STEP + RIM - s, 0) if s else window
            for q in range((RIM + 8) // 8):
                j = s + 8 * q - first
                if 0 <= j < tap_count:
                    total = total + taps[j : j + 1, :] * turned[8 * q : 8 * q + STEP]
        pad[aligned(i, STEP), :] = total
        lane = lax.broadcasted_iota(jnp.int32, (STEP, 128), 1)
        plain = jnp.sum(total, axis=1, keepdims=True)
        square = jnp.sum(total * total, axis=1, keepdims=True)
        cols_st[aligned(i, STEP), :] = jnp.where(
            lane == 0, plain, jnp.where(lane == 1, square, 0.0)
        )

    stat[0] = cols_st[...].T[:8]
    stat_near = remote(stat.at[0], stat.at[1], stat_sem.at[0], stat_sem.at[1], near)
    stat_near.start()

    normalize(lax.rem(t + 1, 4))
    normalize(lax.rem(t + 3, 4))
    stat_near.wait()
    stat[2] = stat[0] + stat[1]
    stat_far = remote(stat.at[2], stat.at[3], stat_sem.at[2], stat_sem.at[3], far)
    stat_far.start()
    down_far[3].start()
    get_sg.wait()
    get_su.wait()
    sacc[...] = jnp.zeros_like(sacc)

    @pl.loop(0, CHUNKS)
    def _(k):
        at = aligned(k, chunk)
        sacc[0] += dot(tok[:, at], wbuf[0, at, :])
        sacc[1] += dot(tok[:, at], wbuf[2, at, :])

    get_own_gate = fetch(expert_gate, wbuf.at[0], 3)
    get_own_up = fetch(expert_up, wbuf.at[2], 4)
    get_own_gate.start()
    get_own_up.start()
    hs[...] = (silu(sacc[0]) * sacc[1]).astype(BF16)

    def outside(j):
        return lax.rem(base + HALF + j, count)

    def forward(g, j):
        source = outside(j)
        return remote(rows.at[g, source], frows.at[g, source], f_send.at[g, j], f_recv.at[g, j], far)

    def forward_some(g, start, stop):
        @pl.loop(start, stop)
        def _(j):
            came(g, outside(j)).wait_recv()
            forward(g, j).start()

    def near_came(g):
        @pl.loop(1, HALF)
        def _(j):
            came(g, base + lax.rem(place_in + j, HALF)).wait_recv()

    def forward_group(g):
        forward_some(g, 0, count - HALF)
        near_came(g)

    def far_ready(g):
        @pl.loop(1, HALF)
        def _(j):
            doubled(g, j).wait()

        @pl.loop(0, count - HALF)
        def _(j):
            forward(g, j).wait()

    def ffn(source, g, slot):
        lhs = source.at[g]
        gate_sum = jnp.zeros((batch, hidden), F32)
        up_sum = jnp.zeros((batch, hidden), F32)

        def step(k, sums):
            at = aligned(k, chunk)
            x = lhs[:, :, at].reshape(batch, chunk)
            return sums[0] + dot(x, wbuf[slot, at, :]), sums[1] + dot(x, wbuf[slot + 2, at, :])

        gate_sum, up_sum = lax.fori_loop(0, CHUNKS, step, (gate_sum, up_sum))
        return (silu(gate_sum) * up_sum).astype(BF16)

    def own_part(g):
        hid[g, 0] = ffn(rows, g, 0)
        hid[g, 2] = ffn(rows, g, 1)

    hidden_far = [
        [
            remote(hfar.at[g, n], hid.at[g, 1 + 2 * n], h_send.at[g, n], h_recv.at[g, n], far)
            for n in range(2)
        ]
        for g in range(groups)
    ]

    def far_part(g):
        far_ready(g)
        for n in range(2):
            hfar[g, n] = ffn(frows, g, n)
            hidden_far[g][n].start()

    def halves(which, lhs, depth):
        @pl.loop(0, tiles)
        def _(i):
            at = aligned(i, TILE)
            for j in range(2):
                block = aligned(2 * j + 1 - core, own)
                ns[j, :, at] = dot(lhs[block, :], opbuf[pl.ds(0, depth), at]).astype(BF16)
            for j in range(2):
                block = aligned(2 * j + core, own)
                kept[which, j, :, at] = dot(lhs[block, :], opbuf[pl.ds(0, depth), at]).astype(BF16)

    to_near = [
        remote(ns, nr.at[which], rs_near.at[which, 0], rs_near.at[which, 1], near) for which in range(2)
    ]
    piece = width // PIECES

    def crossing(which, c, into):
        return remote(
            kept.at[which, 1 - low, :, pl.ds(c * piece, piece)],
            into.at[:, pl.ds(c * piece, piece)],
            rs_far.at[which, 0, c],
            rs_far.at[which, 1, c],
            far,
        )

    shared_cross = [crossing(0, c, arr) for c in range(PIECES)]
    mixer_cross = [crossing(1, c, mix) for c in range(PIECES)]

    def joined(which):
        to_near[which].wait_recv()

        @pl.loop(0, own // 16)
        def _(i):
            at = aligned(i, 16)
            kept[which, 1 - low, at, :] = (
                kept[which, 1 - low, at, :].astype(F32) + nr[which, 1 - low, at, :].astype(F32)
            ).astype(BF16)

    def back(g, to):
        return remote(box.at[g, to], ret.at[g, me], ret_send.at[g], ret_recv.at[g], {"ep": to})

    def products(g):
        others = pl.ds(0, count - 1)
        after = {"ep": lax.rem(me + 1, count)}
        remote(box.at[g, others], rows.at[g, others], go_send.at[g], go_recv.at[g, 0], after).wait_send()

        for n in range(2):
            hidden_far[g][n].wait()

        @pl.loop(0, tiles)
        def _(i):
            at = aligned(i, TILE)
            total = dot(hid[g, 0], dbuf[:, at])
            for piece in range(3):
                total += dot(hid[g, piece + 1], downs[piece, :, at])
            box[g, :, :, at] = total.astype(BF16).reshape(count, UNIT, TILE)

        @pl.loop(1, count)
        def _(j):
            back(g, lax.rem(me + j, count)).start()

        ret[g, me] = box[g, me]

    def combine(g):
        others = pl.ds(0, count - 1)
        after = {"ep": lax.rem(me + 1, count)}
        remote(box.at[g, others], ret.at[g, others], ret_send.at[g], ret_recv.at[g], after).wait()

        def tile(i):
            at = aligned(i, TILE)
            back_rows = ret[g, :, :, at].reshape(batch, TILE)
            total = jnp.zeros((own, TILE), F32)
            for k in range(choice.shape[0]):
                total += dot(choice[k, g], back_rows) * share_cols[:, k : k + 1]
            if g:
                total += total_out[:, at]
            if g == groups - 1:
                arr[:, at] = (total + ended(at).astype(F32)).astype(BF16)
            else:
                total_out[:, at] = total

        if g < groups - 1:
            pl.loop(0, tiles)(tile)
        else:
            for c in range(CHUNKS):
                pl.loop(c * tiles // CHUNKS, (c + 1) * tiles // CHUNKS)(tile)
                put(c).start()

    def put(c):
        return pltpu.make_async_copy(arr.at[:, cols(c)], out_ref.at[:, cols(c)], put_sem.at[c])

    def ended(at, which=0, came_from=arr):
        return (
            kept[which, low, :, at].astype(F32)
            + nr[which, low, :, at].astype(F32)
            + came_from[:, at].astype(F32)
        ).astype(BF16)

    def normed():
        stat_far.wait()
        total = stat[2] + stat[3]
        cols_st[...] = jnp.concatenate([total, jnp.zeros((120, length), F32)], axis=0).T
        channels = pad.shape[1] * 4

        @pl.loop(0, length // STEP)
        def _(i):
            at = aligned(i, STEP)
            average = cols_st[at, 0:1] / channels
            variance = cols_st[at, 1:2] / channels - average * average
            scale = lax.rsqrt(variance + EPSILON)
            v = (pad[at, :] - average) * scale * ln_gain[...] + ln_bias[...]
            act[at, :] = silu(v).astype(BF16)

    def relay(c):
        down_far[c].wait()
        down_on[c].start()

    get_op = fetch(out_proj, opbuf, 5)

    if groups > 1:
        send_rows(1)
        send_doubles(1)
    for g in range(2, groups):
        gather_rows(g)
    forward_group(0)
    relay(0)
    relay(1)
    get_own_gate.wait()
    get_own_up.wait()
    gate_near.wait()
    up_near.wait()
    own_part(0)
    for g in range(2, groups):
        send_rows(g)
        send_doubles(g)
    get_sd.wait()
    halves(0, hs, hidden)
    to_near[0].start()
    get_op.start()
    relay(2)
    normed()
    get_op.wait()
    to_near[0].wait_send()
    halves(1, act, act.shape[1])
    to_near[1].start()
    joined(0)
    shared_cross[0].start()
    far_part(0)
    if groups > 1:
        forward_group(1)
        own_part(1)
    relay(3)
    get_down.wait()
    for c in range(CHUNKS):
        down_near[c].wait()
        down_on[c].wait()
    products(0)
    joined(1)
    def finish_crossing():
        for copy in shared_cross[EARLY + 1 :] + mixer_cross:
            copy.start()

    for g in range(1, groups):
        if g + 2 == groups:
            shared_cross[1].start()
        far_part(g)
        if g + 1 < groups:
            if g + 2 == groups:
                for copy in shared_cross[2 : EARLY + 1]:
                    copy.start()
            forward_group(g + 1)
            own_part(g + 1)
        else:
            finish_crossing()
        products(g)
    if groups < 3:
        for copy in shared_cross[1 : EARLY + 1]:
            copy.start()
    if groups == 1:
        finish_crossing()
    for g in range(groups - 1):
        combine(g)
    to_near[1].wait_send()
    for copy in shared_cross + mixer_cross:
        copy.wait()

    @pl.loop(0, tiles)
    def _(i):
        at = aligned(i, TILE)
        mix[:, at] = ended(at, 1, mix)

    put_mixer = pltpu.make_async_copy(mix, mixer_ref, put_sem.at[CHUNKS])
    put_mixer.start()
    combine(groups - 1)
    put_mixer.wait()
    for c in range(CHUNKS):
        put(c).wait()


def per_device(
    value_in,
    gate_in,
    conv_taps,
    conv_bias,
    ln_gain,
    ln_bias,
    out_proj,
    tokens_b,
    norm_gain,
    routes,
    route_weights,
    expert_gate,
    expert_up,
    expert_down,
    shared_gate,
    shared_up,
    shared_down,
):
    ep_count = lax.axis_size("ep")
    own, top_count = routes.shape
    length, channels = value_in.shape
    width, hidden = tokens_b.shape[1], expert_down.shape[1]
    cap = 3 * own * top_count // (2 * ep_count)
    groups = -(-cap // UNIT)
    batch = ep_count * UNIT
    anywhere = pl.BlockSpec(memory_space=pl.ANY)
    vmem = pl.BlockSpec(memory_space=pltpu.VMEM)
    dma = pltpu.SemaphoreType.DMA
    mail = pltpu.VMEM((groups, ep_count, UNIT, width), BF16)
    return pl.pallas_call(
        kernel,
        out_shape=[jax.ShapeDtypeStruct((own, width), BF16)] * 2,
        in_specs=[anywhere] * 2 + [vmem] * 7 + [anywhere] * 8,
        out_specs=[anywhere] * 2,
        scratch_shapes=[
            pltpu.VMEM((length, channels), BF16),
            pltpu.VMEM((length, channels), BF16),
            pltpu.VMEM((4, width, hidden), BF16),
            pltpu.VMEM((max(channels, hidden), width), BF16),
            pltpu.VMEM((hidden, width), BF16),
            pltpu.VMEM((3, hidden, width), BF16),
            pltpu.VMEM((4 * own, width), BF16),
            mail,
            pltpu.VMEM((groups, HALF, UNIT, width), BF16),
            mail,
            mail,
            mail,
            pltpu.VMEM((length + RIM, channels), F32),
            pltpu.VMEM((length, channels), BF16),
            pltpu.VMEM((4 * own, hidden), BF16),
            pltpu.VMEM((2, own, width), BF16),
            pltpu.VMEM((2, 2, own, width), BF16),
            pltpu.VMEM((2, 2, own, width), BF16),
            pltpu.VMEM((own, width), BF16),
            pltpu.VMEM((own, width), BF16),
            pltpu.VMEM((2, 4 * own, hidden), F32),
            pltpu.VMEM((groups, 4, batch, hidden), BF16),
            pltpu.VMEM((groups, 2, batch, hidden), BF16),
            pltpu.VMEM((own, width), F32),
            pltpu.VMEM((4, 8, length), F32),
            pltpu.VMEM((length, 128), F32),
            pltpu.VMEM((top_count, groups, own, batch), BF16),
            pltpu.VMEM((own, own), F32),
            pltpu.VMEM((groups * batch, own), BF16),
            pltpu.VMEM((top_count, own), jnp.int32),
            dma((9,)),
            dma((CHUNKS + 1,)),
            dma((4,)),
            dma((2,)),
            dma((4,)),
            dma((2,)),
            dma((2,)),
            dma((2,)),
            dma((CHUNKS,)),
            dma((CHUNKS,)),
            dma((2, CHUNKS)),
            dma((2, CHUNKS)),
            dma((2, 2)),
            dma((2, 2, PIECES)),
            dma((groups,)),
            dma((groups, ep_count)),
            dma((groups, HALF)),
            dma((groups, HALF)),
            dma((groups, ep_count - HALF)),
            dma((groups, ep_count - HALF)),
            dma((groups, 2)),
            dma((groups, 2)),
            dma((groups,)),
            dma((groups,)),
        ],
        compiler_params=pltpu.CompilerParams(
            collective_id=0, has_side_effects=True, vmem_limit_bytes=67043328
        ),
    )(
        value_in,
        gate_in,
        conv_taps,
        conv_bias[None],
        ln_gain[None],
        ln_bias[None],
        norm_gain[None],
        routes.T,
        route_weights.T,
        out_proj,
        tokens_b,
        expert_gate[0],
        expert_up[0],
        expert_down[0],
        shared_gate,
        shared_up,
        shared_down,
    )


def solution(mesh):
    return jax.shard_map(
        lambda *args: tuple(per_device(*args)),
        mesh=mesh,
        in_specs=(
            P("ep", "tp"),
            P("ep", "tp"),
            P(None, "tp"),
            P("tp"),
            P("tp"),
            P("tp"),
            P("tp", None),
            P("ep", None),
            P(),
            P(("ep", "tp"), None),
            P(("ep", "tp"), None),
            P("ep", None, "tp"),
            P("ep", None, "tp"),
            P("ep", "tp", None),
            P(None, "tp"),
            P(None, "tp"),
            P("tp", None),
        ),
        out_specs=(P(("ep", "tp"), None), P(("ep", "tp"), None)),
        check_vma=False,
    )
```
